32 devices in a mesh: fs: 4 (over z), rep: 4 (over y, x), tp: 2 (over core).
Axes of the slice: x: 2, y: 2, z: 4, core: 2. Of those that a mesh axis runs over, the one named last changes fastest.
Arguments:
- saved_input: bfloat16 [16384, 2048], P(('fs', 'rep')), may hold values from -6 to 6
- cot_input: bfloat16 [16384, 1024], P(('fs', 'rep'), 'tp'), may hold values from -0.046875 to 0.046875
- cot_gate: bfloat16 [16384, 1024], P(('fs', 'rep'), 'tp'), may hold values from -0.046875 to 0.046875
- in_master: float32 [2048, 1024], P('fs', 'tp'), may hold values from -3 to 3
- gate_master: float32 [2048, 1024], P('fs', 'tp'), may hold values from -3 to 3
- in_factor: bfloat16 [2048, 256], P('fs'), may hold values from -0.125 to 0.125
- gate_factor: bfloat16 [2048, 256], P('fs'), may hold values from -0.125 to 0.125
- in_first: float32 [256, 1024], P('fs', 'tp'), may hold values from -6 to 6
- in_second: float32 [256, 1024], P('fs', 'tp'), may hold values from 0.5 to 2
- gate_first: float32 [256, 1024], P('fs', 'tp'), may hold values from -6 to 6
- gate_second: float32 [256, 1024], P('fs', 'tp'), may hold values from 0.5 to 2
Outputs:
- in_master_new: float32 [2048, 1024], P('fs', 'tp')
- gate_master_new: float32 [2048, 1024], P('fs', 'tp')
- in_update: float32 [2048, 1024], P('fs', 'tp')
- gate_update: float32 [2048, 1024], P('fs', 'tp')
- in_first_new: float32 [256, 1024], P('fs', 'tp')
- in_second_new: float32 [256, 1024], P('fs', 'tp')
- gate_first_new: float32 [256, 1024], P('fs', 'tp')
- gate_second_new: float32 [256, 1024], P('fs', 'tp')
- in_copy: bfloat16 [2048, 1024], P(None, 'tp')
- gate_copy: bfloat16 [2048, 1024], P(None, 'tp')
The draws below stay inside these ranges and needn't reach their ends.
All inputs are finite; a program needn't handle non-finite values.
Results may differ from the reference program's by a relative error of at most 0.0065.
Values may be sent and summed in bfloat16 or wider, within the bound.
No kernel may reach another device: no remote copies, remote signals or barrier semaphores. Data moves between devices by JAX's collectives and lax.ppermute only.
A program may use at most 64 MiB of HBM per device.

```python
import math
import jax
import jax.numpy as jnp
from jax import lax

D = 2048
W = 1024
RANK = 256
TOKENS = 16384


def steps_of(own_key, shape, pieces, low, top_value):
    level, own = 1.0, jax.random.fold_in(own_key, 6)
    for position, parts in pieces:
        steps = jnp.exp(jax.random.uniform(jax.random.fold_in(own, position), (parts,), jnp.float32, low / len(pieces), top_value / len(pieces)))
        level = level * jnp.repeat(steps, shape[position] // parts).reshape([-1 if axis == position else 1 for axis in range(len(shape))])
    return level


def gaussian(rng, shape, scale, reach, shards=(), kind=jnp.bfloat16):
    gain = steps_of(rng, shape, shards, -0.22, 0.18) if shards else 1.0
    entries = jax.random.normal(rng, shape, jnp.float32) * scale * gain
    return jnp.minimum(jnp.maximum(entries, -reach), reach).astype(kind)


def setup_inputs(seed: int = 0) -> dict:
    keys = jax.random.split(jax.random.key(seed), 12)
    saved_input = gaussian(keys[0], (TOKENS, D), 1.0, 6.0, ((0, 16),))
    cot_input = gaussian(keys[1], (TOKENS, W), TOKENS ** -0.5, 0.046875, ((0, 16), (1, 2)))
    cot_gate = gaussian(keys[2], (TOKENS, W), TOKENS ** -0.5, 0.046875, ((0, 16), (1, 2)))
    in_master = gaussian(keys[3], (D, W), 0.5, 3.0, ((0, 4), (1, 2)), jnp.float32)
    gate_master = gaussian(keys[4], (D, W), 0.5, 3.0, ((0, 4), (1, 2)), jnp.float32)
    in_factor = gaussian(keys[5], (D, RANK), D ** -0.5, 0.125, ((0, 4),))
    gate_factor = gaussian(keys[6], (D, RANK), D ** -0.5, 0.125, ((0, 4),))
    in_first = gaussian(keys[7], (RANK, W), 1.0, 6.0, ((0, 4), (1, 2)), jnp.float32)
    in_second = jnp.clip(jnp.exp(math.log(2.0) - 1.3862944 * jax.random.uniform(keys[8], (RANK, W), jnp.float32) ** steps_of(keys[8], (RANK, W), ((0, 4), (1, 2)), -0.2, 0.2)), 0.5, 2.0)
    gate_first = gaussian(keys[9], (RANK, W), 1.0, 6.0, ((0, 4), (1, 2)), jnp.float32)
    gate_second = jnp.clip(jnp.exp(math.log(2.0) - 1.3862944 * jax.random.uniform(keys[10], (RANK, W), jnp.float32) ** steps_of(keys[10], (RANK, W), ((0, 4), (1, 2)), -0.2, 0.2)), 0.5, 2.0)
    return {"saved_input": saved_input, "cot_input": cot_input, "cot_gate": cot_gate, "in_master": in_master, "gate_master": gate_master, "in_factor": in_factor, "gate_factor": gate_factor, "in_first": in_first, "in_second": in_second, "gate_first": gate_first, "gate_second": gate_second}


def adapt(grad, master, factor, first, second):
    basis = factor.astype(jnp.float32)
    low = jnp.dot(basis.T, grad, precision=lax.Precision.HIGHEST)
    first_new = 0.8 * first + 0.2 * low
    second_new = 0.95 * second + 0.05 * low * low
    normed = first_new / jnp.sqrt(second_new)
    full = jnp.dot(basis, normed, precision=lax.Precision.HIGHEST)
    square = jnp.sum(full * full)
    update = full / jnp.sqrt(square / (D * W) + 0.1)
    master_new = master - 0.05 * update
    return (master_new, update, first_new, second_new, master_new.astype(jnp.bfloat16))

def reference(saved_input, cot_input, cot_gate, in_master, gate_master, in_factor, gate_factor, in_first, in_second, gate_first, gate_second):
    cotangents = jnp.concatenate([cot_input, cot_gate], axis=1)
    span = math.gcd(TOKENS, 8192)
    inputs = saved_input.reshape(TOKENS // span, span, D)
    grads_in = cotangents.reshape(TOKENS // span, span, 2 * W)

    def accumulate(total, pair):
        rows, cots = pair
        part = jnp.dot(rows.astype(jnp.float32).T, cots.astype(jnp.float32), precision=lax.Precision.HIGHEST)
        return (total + part, None)
    grads, _ = lax.scan(accumulate, jnp.zeros((D, 2 * W), jnp.float32), (inputs, grads_in))
    in_out = adapt(grads[:, :W], in_master, in_factor, in_first, in_second)
    gate_out = adapt(grads[:, W:], gate_master, gate_factor, gate_first, gate_second)
    return (in_out[0], gate_out[0], in_out[1], gate_out[1], in_out[2], in_out[3], gate_out[2], gate_out[3], in_out[4], gate_out[4])
```

```python
import functools

import jax
import jax.numpy as jnp
from jax import lax
from jax.experimental import pallas as pl
from jax.experimental.pallas import tpu as pltpu
from jax.sharding import PartitionSpec as P


F32 = jnp.float32
BF16 = jnp.bfloat16
DIRECT = 4
CONTRACT_ROWS = (((0,), (0,)), ((), ()))


def dot(left, right):
    return jnp.dot(left, right, preferred_element_type=F32)


def swap(values, axis, size, step):
    return lax.ppermute(values, axis, [(i, i ^ step) for i in range(size)])


def from_others(values, axis, size):
    if size <= DIRECT:
        return [swap(values, axis, size, k) for k in range(1, size)]
    whole = lax.all_gather(values, axis)
    order = lax.axis_index(axis) ^ jnp.arange(1, size)
    return [jnp.take(whole, order, axis=0).reshape((-1, *values.shape[1:]))]


def full_spec(array):
    return pl.BlockSpec(array.shape, lambda *_: (0,) * array.ndim)


def struct(shape, kind):
    return jax.ShapeDtypeStruct(shape, kind)


def walk(refs, rows):
    k = 0
    for ref in refs:
        for offset in range(0, ref.shape[0], rows):
            k += 1
            yield k, ref, offset


def project(place, x, own, direct, relayed, rep_size):
    tokens, model = x.shape
    rows, rank = own.shape
    part = rows // rep_size
    block = min(256, tokens)
    n_direct = len(direct)

    def body(place_ref, x_ref, own_ref, *refs):
        pieces, (y_ref, whole_ref) = refs[:-2], refs[-2:]

        @pl.when(pl.program_id(0) == 0)
        def _():
            fs, rep = place_ref[0], place_ref[1]
            whole_ref[pl.ds(pl.multiple_of(fs * rows, rows), rows), :] = own_ref[...]
            groups = [(0, pieces[:n_direct])]
            groups += [(j + 1, [piece]) for j, piece in enumerate(pieces[n_direct:])]
            for j, group in groups:
                for k, ref, offset in walk(group, part):
                    start = pl.multiple_of((fs ^ k) * rows + (rep ^ j) * part, part)
                    whole_ref[pl.ds(start, part), :] = ref[offset : offset + part, :]

        y_ref[...] = dot(x_ref[...], whole_ref[...]).astype(BF16)

    operands = (x, own, *direct, *relayed)
    return pl.pallas_call(
        body,
        grid_spec=pltpu.PrefetchScalarGridSpec(
            num_scalar_prefetch=1,
            grid=(tokens // block,),
            in_specs=[pl.BlockSpec((block, model), lambda i, _: (i, 0))] + [full_spec(a) for a in operands[1:]],
            out_specs=[
                pl.BlockSpec((block, rank), lambda i, _: (i, 0)),
                pl.BlockSpec((model, rank), lambda i, _: (0, 0)),
            ],
        ),
        out_shape=[struct((tokens, rank), BF16), struct((model, rank), BF16)],
        name="project",
    )(place, *operands)


def token_sums(place, y_own, y_other, cot_input, cot_gate, fs_size):
    rank = y_own.shape[1]
    width = cot_input.shape[1]
    rows = rank // fs_size
    split = fs_size <= DIRECT

    def body(place_ref, own_ref, other_ref, ci_ref, cg_ref, *refs):
        outs, scratch = refs[:-1], refs[-1]
        first = place_ref[2] == 0
        y_in = jnp.where(first, own_ref[...], other_ref[...])
        y_gate = jnp.where(first, other_ref[...], own_ref[...])
        scratch[:, :width] = lax.dot_general(y_in, ci_ref[...], CONTRACT_ROWS, preferred_element_type=F32)
        scratch[:, width:] = lax.dot_general(y_gate, cg_ref[...], CONTRACT_ROWS, preferred_element_type=F32)
        if not split:
            outs[0][...] = scratch[...].astype(BF16)
            return
        for k, out in enumerate(outs):
            start = pl.multiple_of((place_ref[0] ^ k) * rows, rows)
            out[...] = scratch[pl.ds(start, rows), :].astype(out.dtype)

    if split:
        outs = [struct((rows, 2 * width), BF16 if k else F32) for k in range(fs_size)]
    else:
        outs = [struct((rank, 2 * width), BF16)]
    operands = (y_own, y_other, cot_input, cot_gate)
    return pl.pallas_call(
        body,
        grid_spec=pltpu.PrefetchScalarGridSpec(
            num_scalar_prefetch=1,
            grid=(1,),
            in_specs=[full_spec(a) for a in operands],
            out_specs=[full_spec(o) for o in outs],
            scratch_shapes=[pltpu.VMEM((rank, 2 * width), F32)],
        ),
        out_shape=outs,
        name="token_sums",
    )(place, *operands)


def add_up(parts):
    def body(*refs):
        total = refs[0][...].astype(F32)
        for ref in refs[1:-1]:
            total = total + ref[...].astype(F32)
        refs[-1][...] = total.astype(BF16)

    return pl.pallas_call(body, out_shape=struct(parts[0].shape, BF16), name="add_up")(*parts)


def tree(values):
    while len(values) > 1:
        values = [values[i] + values[i + 1] for i in range(0, len(values), 2)]
    return values[0]


def moments(parts, in_first, in_second, gate_first, gate_second):
    rows, width = in_first.shape
    count = len(parts)

    def body(*refs):
        sums, olds, outs = refs[:count], refs[count : count + 4], refs[count + 4 :]
        low = tree([ref[...].astype(F32) for ref in sums])
        for side in (0, 1):
            part = low[:, side * width : (side + 1) * width]
            first = 0.8 * olds[2 * side][...] + 0.2 * part
            second = 0.95 * olds[2 * side + 1][...] + 0.05 * part * part
            outs[2 * side][...] = first
            outs[2 * side + 1][...] = second
            outs[4][:, side * width : (side + 1) * width] = (first / jnp.sqrt(second)).astype(BF16)

    small = struct((rows, width), F32)
    return pl.pallas_call(
        body,
        out_shape=[small, small, small, small, struct((rows, 2 * width), BF16)],
        name="moments",
    )(*parts, in_first, in_second, gate_first, gate_second)


def flat_rows(values):
    count, rows, width = values.shape
    if rows % 16:
        return values.astype(F32).reshape(count * rows, width).astype(BF16)
    return values.reshape(count * rows, width)


def squares(place, normed, others, u_own, u_other, fs_size):
    rows, both = normed.shape
    width = both // 2
    model = u_own.shape[0]
    block = min(512, model)

    def body(place_ref, normed_ref, *refs):
        pieces, (own_ref, other_ref, all_ref, sum_ref) = refs[:-4], refs[-4:]
        fs = place_ref[0]
        all_ref[fs] = normed_ref[...]
        for k, ref, offset in walk(pieces, rows):
            all_ref[fs ^ k] = ref[offset : offset + rows, :]
        first = place_ref[2] == 0
        whole = flat_rows(all_ref[...])
        totals = [jnp.zeros((8, width), F32), jnp.zeros((8, width), F32)]
        for start in range(0, model, block):
            own, other = own_ref[start : start + block, :], other_ref[start : start + block, :]
            for side, u in ((0, jnp.where(first, own, other)), (1, jnp.where(first, other, own))):
                full = dot(u, whole[:, side * width : (side + 1) * width])
                totals[side] = totals[side] + jnp.sum((full * full).reshape(block // 8, 8, width), axis=0)
        sum_ref[:8, :] = jnp.broadcast_to(jnp.sum(totals[0]), (8, 128))
        sum_ref[8:, :] = jnp.broadcast_to(jnp.sum(totals[1]), (8, 128))

    operands = (normed, *others, u_own, u_other)
    outs = [struct((fs_size, rows, both), BF16), struct((16, 128), F32)]
    return pl.pallas_call(
        body,
        grid_spec=pltpu.PrefetchScalarGridSpec(
            num_scalar_prefetch=1,
            grid=(1,),
            in_specs=[full_spec(a) for a in operands],
            out_specs=[full_spec(o) for o in outs],
        ),
        out_shape=outs,
        name="squares",
    )(place, *operands)


def finish(place, sum_own, sum_other, normed, u_own, u_other, in_master, gate_master, gathered, entries):
    rows, width = in_master.shape
    model, rank = u_own.shape
    fs_size = model // rows
    per = gathered.shape[0] // fs_size
    part = rows // per

    def body(place_ref, so_ref, st_ref, n_ref, uo_ref, ut_ref, im_ref, gm_ref, old_ref, *outs):
        first = place_ref[2] == 0
        whole = flat_rows(n_ref[...])
        own, other = uo_ref[...], ut_ref[...]
        for side, u in ((0, jnp.where(first, own, other)), (1, jnp.where(first, other, own))):
            square = so_ref[8 * side : 8 * side + 1, :1] + st_ref[8 * side : 8 * side + 1, :1]
            scale = lax.rsqrt(square / entries + 0.1)
            update = dot(u, whole[:, side * width : (side + 1) * width]) * scale
            old = old_ref[:, side].astype(F32).reshape(rows, width)
            outs[4 + side][...] = (old - 0.05 * update).astype(BF16)

            @pl.when(pl.program_id(0) == 0)
            def _():
                outs[2 + side][...] = update
                outs[side][...] = (im_ref, gm_ref)[side][...] - 0.05 * update

    def at(i, place_ref):
        return place_ref[0] ^ i

    same = pl.BlockSpec((rows, width), lambda i, _: (0, 0))
    spread = pl.BlockSpec((rows, width), lambda i, p: (at(i, p), 0))
    factor = pl.BlockSpec((rows, rank), lambda i, p: (at(i, p), 0))
    small, big = struct((rows, width), F32), struct((model, width), BF16)
    return pl.pallas_call(
        body,
        grid_spec=pltpu.PrefetchScalarGridSpec(
            num_scalar_prefetch=1,
            grid=(fs_size,),
            in_specs=[
                full_spec(sum_own),
                full_spec(sum_other),
                full_spec(normed),
                factor,
                factor,
                same,
                same,
                pl.BlockSpec((per, 2, part, width), lambda i, p: (at(i, p), 0, 0, 0)),
            ],
            out_specs=[same, same, same, same, spread, spread],
        ),
        out_shape=[small, small, small, small, big, big],
        name="finish",
    )(place, sum_own, sum_other, normed, u_own, u_other, in_master, gate_master, gathered)


def on_device(
    sizes,
    saved_input,
    cot_input,
    cot_gate,
    in_master,
    gate_master,
    in_factor,
    gate_factor,
    in_first,
    in_second,
    gate_first,
    gate_second,
):
    fs_size, rep_size, tp_size = sizes
    rows, width = in_master.shape
    rank = in_factor.shape[1]
    part = rows // rep_size
    fs, rep, tp = (lax.axis_index(name) for name in ("fs", "rep", "tp"))
    place = jnp.stack([fs, rep, tp]).astype(jnp.int32)

    def own_part(values):
        return lax.dynamic_slice_in_dim(values, rep * part, part, 0)

    own = jnp.where(tp == 0, in_factor, gate_factor)
    direct = from_others(jnp.where(tp == 0, own_part(in_factor), own_part(gate_factor)), "fs", fs_size)
    stacked = jnp.concatenate(direct, axis=0)
    relayed = from_others(stacked, "rep", rep_size)
    old = jnp.stack([own_part(in_master), own_part(gate_master)]).astype(BF16)
    gathered = lax.all_gather(old[None], ("fs", "rep"), axis=0, tiled=True)

    y_own, u_own = project(place, saved_input, own, direct, relayed, rep_size)
    y_other = swap(y_own, "tp", tp_size, 1)
    u_other = swap(u_own, "tp", tp_size, 1)
    sums = token_sums(place, y_own, y_other, cot_input, cot_gate, fs_size)
    if fs_size <= DIRECT:
        parts = [sums[0]] + [swap(sums[k], "fs", fs_size, k) for k in range(1, fs_size)]
        partial = add_up(parts)
    else:
        partial = lax.psum_scatter(sums[0], "fs", scatter_dimension=0, tiled=True)
    parts = [partial] + from_others(partial, "rep", rep_size)
    *new, normed = moments(parts, in_first, in_second, gate_first, gate_second)
    others = from_others(normed, "fs", fs_size)
    whole, sum_own = squares(place, normed, others, u_own, u_other, fs_size)
    sum_other = swap(sum_own, "tp", tp_size, 1)
    entries = float(rows * fs_size * width * tp_size)
    head = finish(place, sum_own, sum_other, whole, u_own, u_other, in_master, gate_master, gathered, entries)
    return (*head[:4], *new, *head[4:])


def solution(mesh):
    sizes = tuple(mesh.shape[name] for name in ("fs", "rep", "tp"))
    owned, moment = P("fs", "tp"), P("fs", "tp")
    return jax.shard_map(
        functools.partial(on_device, sizes),
        mesh=mesh,
        in_specs=(
            P(("fs", "rep"), None),
            P(("fs", "rep"), "tp"),
            P(("fs", "rep"), "tp"),
            owned,
            owned,
            P("fs", None),
            P("fs", None),
            moment,
            moment,
            moment,
            moment,
        ),
        out_specs=(owned,) * 4 + (moment,) * 4 + (P(None, "tp"),) * 2,
        check_vma=False,
    )
```

```python
import functools

import jax
import jax.numpy as jnp
from jax import lax
from jax.experimental import pallas as pl
from jax.experimental.pallas import tpu as pltpu
from jax.sharding import PartitionSpec as P


F32 = jnp.float32
BF16 = jnp.bfloat16
DIRECT = 4
CONTRACT_ROWS = (((0,), (0,)), ((), ()))


def dot(left, right):
    return jnp.dot(left, right, preferred_element_type=F32)


def swap(values, axis, size, step):
    return lax.ppermute(values, axis, [(i, i ^ step) for i in range(size)])


def from_others(values, axis, size):
    if size <= DIRECT:
        return [swap(values, axis, size, k) for k in range(1, size)]
    whole = lax.all_gather(values, axis)
    order = lax.axis_index(axis) ^ jnp.arange(1, size)
    return [jnp.take(whole, order, axis=0).reshape((-1, *values.shape[1:]))]


def one_step(operands, n_outs, scratch=(), out_space=pltpu.VMEM):
    return pltpu.PrefetchScalarGridSpec(
        num_scalar_prefetch=1,
        grid=(),
        in_specs=[pl.BlockSpec(memory_space=pltpu.VMEM)] * len(operands),
        out_specs=[pl.BlockSpec(memory_space=out_space)] * n_outs,
        scratch_shapes=scratch,
    )


def grant(mib):
    return pltpu.CompilerParams(vmem_limit_bytes=mib << 20)


def struct(shape, kind):
    return jax.ShapeDtypeStruct(shape, kind)


def walk(refs, rows):
    k = 0
    for ref in refs:
        for offset in range(0, ref.shape[0], rows):
            k += 1
            yield k, ref, offset


def stage(values):
    def body(in_ref, out_ref, sem):
        copy = pltpu.make_async_copy(in_ref, out_ref, sem)
        copy.start()
        copy.wait()

    return pl.pallas_call(
        body,
        in_specs=[pl.BlockSpec(memory_space=pltpu.HBM)],
        out_specs=pl.BlockSpec(memory_space=pltpu.VMEM),
        out_shape=struct(values.shape, values.dtype),
        scratch_shapes=[pltpu.SemaphoreType.DMA],
        compiler_params=grant(10),
        name="stage",
    )(values)


def project(place, x, in_factor, gate_factor, direct, relayed, rep_size):
    tokens, model = x.shape
    rows, rank = in_factor.shape
    part = rows // rep_size
    n_direct = len(direct)

    def body(place_ref, x_ref, in_ref, gate_ref, *refs):
        pieces, (y_ref, whole_ref) = refs[:-2], refs[-2:]
        fs, rep = place_ref[0], place_ref[1]
        own = jnp.where(place_ref[2] == 0, in_ref[...], gate_ref[...])
        whole_ref[pl.ds(pl.multiple_of(fs * rows, rows), rows), :] = own
        groups = [(0, pieces[:n_direct])]
        groups += [(j + 1, [piece]) for j, piece in enumerate(pieces[n_direct:])]
        for j, group in groups:
            for k, ref, offset in walk(group, part):
                start = pl.multiple_of((fs ^ k) * rows + (rep ^ j) * part, part)
                whole_ref[pl.ds(start, part), :] = ref[offset : offset + part, :]
        y_ref[...] = dot(x_ref[...], whole_ref[...]).astype(BF16)

    operands = (x, in_factor, gate_factor, *direct, *relayed)
    return pl.pallas_call(
        body,
        grid_spec=one_step(operands, 2),
        out_shape=[struct((tokens, rank), BF16), struct((model, rank), BF16)],
        compiler_params=grant(12),
        name="project",
    )(place, *operands)


def token_sums(place, y_own, y_other, cot_input, cot_gate, fs_size):
    rank = y_own.shape[1]
    width = cot_input.shape[1]
    rows = rank // fs_size
    split = fs_size <= DIRECT

    def body(place_ref, own_ref, other_ref, ci_ref, cg_ref, *refs):
        outs, scratch = refs[:-1], refs[-1]
        first = place_ref[2] == 0
        y_in = jnp.where(first, own_ref[...], other_ref[...])
        y_gate = jnp.where(first, other_ref[...], own_ref[...])
        scratch[:, :width] = lax.dot_general(y_in, ci_ref[...], CONTRACT_ROWS, preferred_element_type=F32)
        scratch[:, width:] = lax.dot_general(y_gate, cg_ref[...], CONTRACT_ROWS, preferred_element_type=F32)
        if not split:
            outs[0][...] = scratch[...].astype(BF16)
            return
        for k, out in enumerate(outs):
            start = pl.multiple_of((place_ref[0] ^ k) * rows, rows)
            out[...] = scratch[pl.ds(start, rows), :].astype(out.dtype)

    if split:
        outs = [struct((rows, 2 * width), BF16 if k else F32) for k in range(fs_size)]
    else:
        outs = [struct((rank, 2 * width), BF16)]
    operands = (y_own, y_other, cot_input, cot_gate)
    return pl.pallas_call(
        body,
        grid_spec=one_step(operands, len(outs), [pltpu.VMEM((rank, 2 * width), F32)]),
        out_shape=outs,
        compiler_params=grant(10),
        name="token_sums",
    )(place, *operands)


def add_up(parts):
    def body(*refs):
        total = refs[0][...].astype(F32)
        for ref in refs[1:-1]:
            total = total + ref[...].astype(F32)
        refs[-1][...] = total.astype(BF16)

    return pl.pallas_call(body, out_shape=struct(parts[0].shape, BF16), compiler_params=grant(3), name="add_up")(*parts)


def tree(values):
    while len(values) > 1:
        values = [values[i] + values[i + 1] for i in range(0, len(values), 2)]
    return values[0]


def moments(parts, in_first, in_second, gate_first, gate_second):
    rows, width = in_first.shape
    count = len(parts)

    def body(*refs):
        sums, olds, outs = refs[:count], refs[count : count + 4], refs[count + 4 :]
        low = tree([ref[...].astype(F32) for ref in sums])
        for side in (0, 1):
            part = low[:, side * width : (side + 1) * width]
            first = 0.8 * olds[2 * side][...] + 0.2 * part
            second = 0.95 * olds[2 * side + 1][...] + 0.05 * part * part
            outs[2 * side][...] = first
            outs[2 * side + 1][...] = second
            outs[4][:, side * width : (side + 1) * width] = (first / jnp.sqrt(second)).astype(BF16)

    small = struct((rows, width), F32)
    return pl.pallas_call(
        body,
        out_shape=[small, small, small, small, struct((rows, 2 * width), BF16)],
        compiler_params=grant(4),
        name="moments",
    )(*parts, in_first, in_second, gate_first, gate_second)


def flat_rows(values):
    count, rows, width = values.shape
    if rows % 16:
        return values.astype(F32).reshape(count * rows, width).astype(BF16)
    return values.reshape(count * rows, width)


def gram(place, u_own, u_other):
    rank = u_own.shape[1]

    def body(place_ref, own_ref, other_ref, out_ref):
        first = place_ref[2] == 0
        own, other = own_ref[...], other_ref[...]
        for side, u in ((0, jnp.where(first, own, other)), (1, jnp.where(first, other, own))):
            products = lax.dot_general(u, u, CONTRACT_ROWS, preferred_element_type=F32)
            upper = products.astype(BF16)
            out_ref[2 * side] = upper
            out_ref[2 * side + 1] = (products - upper.astype(F32)).astype(BF16)

    operands = (u_own, u_other)
    return pl.pallas_call(
        body,
        grid_spec=one_step(operands, 1),
        out_shape=[struct((4, rank, rank), BF16)],
        compiler_params=grant(8),
        cost_estimate=pl.CostEstimate(flops=4 * u_own.shape[0] * rank * rank, bytes_accessed=0, transcendentals=0),
        name="gram",
    )(place, *operands)[0]


def squares(place, normed, others, products, fs_size):
    rows, both = normed.shape
    width = both // 2

    def body(place_ref, normed_ref, *refs):
        pieces, (gram_ref, all_ref, sum_ref) = refs[:-3], refs[-3:]
        fs = place_ref[0]
        all_ref[fs] = normed_ref[...]
        for k, ref, offset in walk(pieces, rows):
            all_ref[fs ^ k] = ref[offset : offset + rows, :]
        whole = flat_rows(all_ref[...])
        for side in (0, 1):
            part = whole[:, side * width : (side + 1) * width]
            image = dot(gram_ref[2 * side], part) + dot(gram_ref[2 * side + 1], part)
            total = jnp.sum(part.astype(F32) * image)
            sum_ref[8 * side : 8 * side + 8, :] = jnp.broadcast_to(total, (8, 128))

    operands = (normed, *others, products)
    return pl.pallas_call(
        body,
        grid_spec=one_step(operands, 2),
        out_shape=[struct((fs_size, rows, both), BF16), struct((16, 128), F32)],
        compiler_params=grant(6),
        name="squares",
    )(place, *operands)


def finish(place, sum_own, sum_other, normed, u_own, u_other, in_master, gate_master, direct, relayed, entries):
    rows, width = in_master.shape
    model = u_own.shape[0]
    fs_size = model // rows
    rep_size = 1 + len(relayed[0])
    part = rows // rep_size
    n_direct = len(direct)

    def body(place_ref, so_ref, st_ref, n_ref, uo_ref, ut_ref, im_ref, gm_ref, *refs):
        olds, refs = refs[: n_direct + 2 * (rep_size - 1)], refs[n_direct + 2 * (rep_size - 1) :]
        outs, (mine, spread, work, sems) = refs[:6], refs[6:]
        fs, rep = place_ref[0], place_ref[1]
        first = place_ref[2] == 0
        whole = flat_rows(n_ref[...])
        copies = []

        def send(source, target):
            copy = pltpu.make_async_copy(source, target, sems.at[len(copies)])
            copy.start()
            copies.append(copy)

        pieces = [None] + [(ref, offset) for _, ref, offset in walk(olds[:n_direct], 2 * part)]
        for i in range(fs_size):
            block = pl.ds(pl.multiple_of((fs ^ i) * rows, rows), rows)
            own, other = uo_ref[block, :], ut_ref[block, :]
            for side, u in ((0, jnp.where(first, own, other)), (1, jnp.where(first, other, own))):
                square = so_ref[8 * side : 8 * side + 1, :1] + st_ref[8 * side : 8 * side + 1, :1]
                scale = lax.rsqrt(square / entries + 0.1)
                update = dot(u, whole[:, side * width : (side + 1) * width]) * scale
                target = spread.at[2 * i + side]
                if i == 0:
                    old = (im_ref, gm_ref)[side][...]
                    mine[2 + side] = update
                    send(mine.at[2 + side], outs[2 + side])
                    mine[side] = old - 0.05 * update
                    send(mine.at[side], outs[side])
                    target[...] = (old.astype(BF16).astype(F32) - 0.05 * update).astype(BF16)
                else:
                    work[...] = update
                    for j in range(rep_size):
                        at = pl.ds(pl.multiple_of((rep ^ j) * part, part), part)
                        if j == 0:
                            ref, offset = pieces[i]
                            old = ref[offset + side * part : offset + (side + 1) * part, :]
                        else:
                            ref = olds[n_direct + side * (rep_size - 1) + j - 1]
                            old = ref[(i - 1) * part : i * part, :]
                        target[at, :] = (old.astype(F32) - 0.05 * work[at, :]).astype(BF16)
                send(target, outs[4 + side].at[block, :])
        for copy in copies:
            copy.wait()

    operands = (sum_own, sum_other, normed, u_own, u_other, in_master, gate_master, *direct, *relayed[0], *relayed[1])
    small, big = struct((rows, width), F32), struct((model, width), BF16)
    scratch = [
        pltpu.VMEM((4, rows, width), F32),
        pltpu.VMEM((2 * fs_size, rows, width), BF16),
        pltpu.VMEM((rows, width), F32),
        pltpu.SemaphoreType.DMA((4 + 2 * fs_size,)),
    ]
    return pl.pallas_call(
        body,
        grid_spec=one_step(operands, 6, scratch, pltpu.HBM),
        out_shape=[small, small, small, small, big, big],
        compiler_params=grant(26),
        name="finish",
    )(place, *operands)


def layer(
    sizes,
    saved_input,
    cot_input,
    cot_gate,
    in_master,
    gate_master,
    in_factor,
    gate_factor,
    in_first,
    in_second,
    gate_first,
    gate_second,
):
    fs_size, rep_size, tp_size = sizes
    rows, width = in_master.shape
    part = rows // rep_size
    fs, rep, tp = (lax.axis_index(name) for name in ("fs", "rep", "tp"))
    place = jnp.stack([fs, rep, tp]).astype(jnp.int32)

    def own_part(values):
        return lax.dynamic_slice_in_dim(values, rep * part, part, 0)

    def after(values, *others):
        return lax.optimization_barrier((values, *others))[0]

    sent = jnp.where(tp == 0, own_part(in_factor), own_part(gate_factor))
    direct = from_others(sent, "fs", fs_size)
    x = stage(saved_input)
    relayed = from_others(jnp.concatenate(direct, axis=0), "rep", rep_size)
    old = jnp.concatenate([own_part(in_master), own_part(gate_master)], axis=0).astype(BF16)
    old_direct = from_others(after(old, *direct), "fs", fs_size)

    y_own, u_own = project(place, x, in_factor, gate_factor, direct, relayed, rep_size)
    y_other = swap(y_own, "tp", tp_size, 1)
    u_other = swap(u_own, "tp", tp_size, 1)
    sums = token_sums(place, y_own, y_other, cot_input, cot_gate, fs_size)
    if fs_size <= DIRECT:
        parts = [sums[0]] + [swap(sums[k], "fs", fs_size, k) for k in range(1, fs_size)]
    else:
        parts = [lax.psum_scatter(sums[0], "fs", scatter_dimension=0, tiled=True)]
    products = gram(place, after(u_own, sums[-1]), u_other)
    partial = add_up(parts)

    def side_of(side, cue):
        ready = lax.optimization_barrier((*old_direct, cue))[:-1]
        return jnp.concatenate(
            [values.reshape(-1, 2, part, width)[:, side].reshape(-1, width) for values in ready], axis=0
        )

    old_in = from_others(side_of(0, sums[-1]), "rep", rep_size)
    parts = [partial] + from_others(partial, "rep", rep_size)
    *new, normed = moments(parts, in_first, in_second, gate_first, gate_second)
    others = from_others(normed, "fs", fs_size)
    old_gate = from_others(side_of(1, normed), "rep", rep_size)
    whole, sum_own = squares(place, normed, others, products, fs_size)
    sum_other = swap(sum_own, "tp", tp_size, 1)
    entries = float(rows * fs_size * width * tp_size)
    olds = (in_master, gate_master, old_direct, (old_in, old_gate))
    head = finish(place, sum_own, sum_other, whole, u_own, u_other, *olds, entries)
    return (*head[:4], *new, *head[4:])


def solution(mesh):
    sizes = tuple(mesh.shape[name] for name in ("fs", "rep", "tp"))
    owned, moment = P("fs", "tp"), P("fs", "tp")
    step = jax.shard_map(
        functools.partial(layer, sizes),
        mesh=mesh,
        in_specs=(
            P(("fs", "rep"), None),
            P(("fs", "rep"), "tp"),
            P(("fs", "rep"), "tp"),
            owned,
            owned,
            P("fs", None),
            P("fs", None),
            moment,
            moment,
            moment,
            moment,
        ),
        out_specs=(owned,) * 4 + (moment,) * 4 + (P(None, "tp"),) * 2,
        check_vma=False,
    )
    if max(sizes) > DIRECT:
        return step
    return step
```

```python
import functools

import jax
import jax.numpy as jnp
from jax import lax
from jax.experimental import pallas as pl
from jax.experimental.pallas import tpu as pltpu
from jax.sharding import PartitionSpec as P


F32 = jnp.float32
BF16 = jnp.bfloat16
DIRECT = 4
CONTRACT_ROWS = (((0,), (0,)), ((), ()))


def dot(left, right):
    return jnp.dot(left, right, preferred_element_type=F32)


def swap(values, axis, size, step):
    return lax.ppermute(values, axis, [(i, i ^ step) for i in range(size)])


def from_others(values, axis, size):
    if size <= DIRECT:
        return [swap(values, axis, size, k) for k in range(1, size)]
    whole = lax.all_gather(values, axis)
    order = lax.axis_index(axis) ^ jnp.arange(1, size)
    return [jnp.take(whole, order, axis=0).reshape((-1, *values.shape[1:]))]


def one_step(operands, n_outs, scratch=(), out_space=pltpu.VMEM):
    return pltpu.PrefetchScalarGridSpec(
        num_scalar_prefetch=1,
        grid=(),
        in_specs=[pl.BlockSpec(memory_space=pltpu.VMEM)] * len(operands),
        out_specs=[pl.BlockSpec(memory_space=out_space)] * n_outs,
        scratch_shapes=scratch,
    )


def grant(mib):
    return pltpu.CompilerParams(vmem_limit_bytes=mib << 20)


def struct(shape, kind):
    return jax.ShapeDtypeStruct(shape, kind)


def walk(refs, rows):
    k = 0
    for ref in refs:
        for offset in range(0, ref.shape[0], rows):
            k += 1
            yield k, ref, offset


def stage(values):
    def body(in_ref, out_ref, sem):
        copy = pltpu.make_async_copy(in_ref, out_ref, sem)
        copy.start()
        copy.wait()

    return pl.pallas_call(
        body,
        in_specs=[pl.BlockSpec(memory_space=pltpu.HBM)],
        out_specs=pl.BlockSpec(memory_space=pltpu.VMEM),
        out_shape=struct(values.shape, values.dtype),
        scratch_shapes=[pltpu.SemaphoreType.DMA],
        compiler_params=grant(10),
        name="stage",
    )(values)


def project(place, x, in_factor, gate_factor, direct, relayed, rep_size):
    tokens, model = x.shape
    rows, rank = in_factor.shape
    part = rows // rep_size
    n_direct = len(direct)

    def body(place_ref, x_ref, in_ref, gate_ref, *refs):
        pieces, (y_ref, whole_ref) = refs[:-2], refs[-2:]
        fs, rep = place_ref[0], place_ref[1]
        own = jnp.where(place_ref[2] == 0, in_ref[...], gate_ref[...])
        whole_ref[pl.ds(pl.multiple_of(fs * rows, rows), rows), :] = own
        groups = [(0, pieces[:n_direct])]
        groups += [(j + 1, [piece]) for j, piece in enumerate(pieces[n_direct:])]
        for j, group in groups:
            for k, ref, offset in walk(group, part):
                start = pl.multiple_of((fs ^ k) * rows + (rep ^ j) * part, part)
                whole_ref[pl.ds(start, part), :] = ref[offset : offset + part, :]
        y_ref[...] = dot(x_ref[...], whole_ref[...]).astype(BF16)

    operands = (x, in_factor, gate_factor, *direct, *relayed)
    return pl.pallas_call(
        body,
        grid_spec=one_step(operands, 2),
        out_shape=[struct((tokens, rank), BF16), struct((model, rank), BF16)],
        compiler_params=grant(12),
        name="project",
    )(place, *operands)


def token_sums(place, y_own, y_other, cot_input, cot_gate, rep_size):
    rank = y_own.shape[1]
    width = cot_input.shape[1]
    columns = 2 * width // rep_size

    def body(place_ref, own_ref, other_ref, ci_ref, cg_ref, *refs):
        outs, scratch = refs[:-1], refs[-1]
        first = place_ref[2] == 0
        y_in = jnp.where(first, own_ref[...], other_ref[...])
        y_gate = jnp.where(first, other_ref[...], own_ref[...])
        for side, (y, ref) in enumerate(((y_in, ci_ref), (y_gate, cg_ref))):
            sums = lax.dot_general(y, ref[...], CONTRACT_ROWS, preferred_element_type=F32)
            for q in range(rep_size // 2):
                scratch[side * (rep_size // 2) + q] = sums[:, q * columns : (q + 1) * columns]
        for j, out in enumerate(outs):
            out[...] = scratch[place_ref[1] ^ j].astype(out.dtype)

    outs = [struct((rank, columns), BF16 if j else F32) for j in range(rep_size)]
    operands = (y_own, y_other, cot_input, cot_gate)
    return pl.pallas_call(
        body,
        grid_spec=one_step(operands, len(outs), [pltpu.VMEM((rep_size, rank, columns), F32)]),
        out_shape=outs,
        compiler_params=grant(10),
        name="token_sums",
    )(place, *operands)


def add_up(place, parts, fs_size):
    rank, columns = parts[0].shape
    rows = rank // fs_size
    split = fs_size <= DIRECT

    def body(place_ref, *refs):
        sums, outs, scratch = refs[: len(parts)], refs[len(parts) : -1], refs[-1]
        total = tree([ref[...].astype(F32) for ref in sums])
        if not split:
            outs[0][...] = total.astype(BF16)
            return
        for k in range(fs_size):
            scratch[k] = total[k * rows : (k + 1) * rows, :]
        for k, out in enumerate(outs):
            out[...] = scratch[place_ref[0] ^ k].astype(out.dtype)

    outs = [struct((rank, columns), BF16)]
    if split:
        outs = [struct((rows, columns), BF16 if k else F32) for k in range(fs_size)]
    return pl.pallas_call(
        body,
        grid_spec=one_step(parts, len(outs), [pltpu.VMEM((fs_size, rows, columns), F32)]),
        out_shape=outs,
        compiler_params=grant(4),
        name="add_up",
    )(place, *parts)


def tree(values):
    while len(values) > 1:
        values = [sum(values[i : i + 2][1:], values[i]) for i in range(0, len(values), 2)]
    return values[0]


def advance(first, second, low):
    return 0.8 * first + 0.2 * low, 0.95 * second + 0.05 * low * low


def norm_block(place, parts, in_first, in_second, gate_first, gate_second):
    rows, columns = parts[0].shape
    width = in_first.shape[1]
    count = len(parts)

    def body(place_ref, *refs):
        sums, (fi, si, fg, sg, low_ref, normed_ref) = refs[:count], refs[count:]
        low = tree([ref[...].astype(F32) for ref in sums]).astype(BF16)
        low_ref[...] = low
        start = place_ref[1] * columns
        at = pl.ds(pl.multiple_of(lax.rem(start, width), columns), columns)
        is_in = start < width
        old_first = jnp.where(is_in, fi[:, at], fg[:, at])
        old_second = jnp.where(is_in, si[:, at], sg[:, at])
        first, second = advance(old_first, old_second, low.astype(F32))
        normed_ref[...] = (first / jnp.sqrt(second)).astype(BF16)

    operands = (*parts, in_first, in_second, gate_first, gate_second)
    block = struct((rows, columns), BF16)
    return pl.pallas_call(
        body,
        grid_spec=one_step(operands, 2),
        out_shape=[block, block],
        compiler_params=grant(3),
        name="norm_block",
    )(place, *operands)


def moments(place, low, others, in_first, in_second, gate_first, gate_second):
    rows, width = in_first.shape
    columns = low.shape[1]
    count = 1 + len(others)

    def body(place_ref, *refs):
        lows, olds, outs, scratch = refs[:count], refs[count : count + 4], refs[count + 4 : -1], refs[-1]
        for j, ref in enumerate(lows):
            start = (place_ref[1] ^ j) * columns
            at = pl.ds(pl.multiple_of(start, columns), columns)
            scratch[:, at] = ref[-rows:, :].astype(F32)
        for side in (0, 1):
            part = scratch[:, side * width : (side + 1) * width]
            new = advance(olds[2 * side][...], olds[2 * side + 1][...], part)
            outs[2 * side][...], outs[2 * side + 1][...] = new

    operands = (low, *others, in_first, in_second, gate_first, gate_second)
    return pl.pallas_call(
        body,
        grid_spec=one_step(operands, 4, [pltpu.VMEM((rows, 2 * width), F32)]),
        out_shape=[struct((rows, width), F32)] * 4,
        compiler_params=grant(4),
        name="moments",
    )(place, *operands)


def flat_rows(values):
    count, rows, width = values.shape
    if rows % 16:
        return values.astype(F32).reshape(count * rows, width).astype(BF16)
    return values.reshape(count * rows, width)


def gram(place, u_own, u_other):
    rank = u_own.shape[1]

    def body(place_ref, own_ref, other_ref, out_ref):
        first = place_ref[2] == 0
        own, other = own_ref[...], other_ref[...]
        for side, u in ((0, jnp.where(first, own, other)), (1, jnp.where(first, other, own))):
            products = lax.dot_general(u, u, CONTRACT_ROWS, preferred_element_type=F32)
            upper = products.astype(BF16)
            out_ref[2 * side] = upper
            out_ref[2 * side + 1] = (products - upper.astype(F32)).astype(BF16)

    operands = (u_own, u_other)
    return pl.pallas_call(
        body,
        grid_spec=one_step(operands, 1),
        out_shape=[struct((4, rank, rank), BF16)],
        compiler_params=grant(8),
        cost_estimate=pl.CostEstimate(flops=4 * u_own.shape[0] * rank * rank, bytes_accessed=0, transcendentals=0),
        name="gram",
    )(place, *operands)[0]


def squares(place, blocks, products, fs_size, width):
    total, columns = blocks[0].shape
    rows = total // (fs_size + 1)

    def body(place_ref, *refs):
        pieces, (gram_ref, all_ref, sum_ref) = refs[:-3], refs[-3:]
        fs, rep = place_ref[0], place_ref[1]
        for j, ref in enumerate(pieces):
            start = (rep ^ j) * columns
            side = start // width
            at = pl.ds(pl.multiple_of(lax.rem(start, width), columns), columns)
            for k in range(fs_size):
                all_ref[side, fs ^ k, :, at] = ref[k * rows : (k + 1) * rows, :]
        for side in (0, 1):
            part = flat_rows(all_ref[side])
            image = dot(gram_ref[2 * side], part) + dot(gram_ref[2 * side + 1], part)
            total = jnp.sum(part.astype(F32) * image)
            sum_ref[8 * side : 8 * side + 8, :] = jnp.broadcast_to(total, (8, 128))

    operands = (*blocks, products)
    return pl.pallas_call(
        body,
        grid_spec=one_step(operands, 2),
        out_shape=[struct((2, fs_size, rows, width), BF16), struct((16, 128), F32)],
        compiler_params=grant(6),
        name="squares",
    )(place, *operands)


def finish(place, sum_own, sum_other, normed, u_own, u_other, in_master, gate_master, halves, in_rest, gate_rest, rep_size, entries):
    rows, width = in_master.shape
    model = u_own.shape[0]
    fs_size = model // rows
    half = rows // 2
    count, parts = len(halves), len(in_rest)

    def body(place_ref, so_ref, st_ref, n_ref, uo_ref, ut_ref, im_ref, gm_ref, *refs):
        olds, refs = refs[: count + 2 * parts], refs[count + 2 * parts :]
        outs, (mine, spread, sems) = refs[:6], refs[6:]
        fs = place_ref[0]
        held = half_of(place_ref[1], rep_size)
        first = place_ref[2] == 0
        whole = [flat_rows(n_ref[side]) for side in (0, 1)]
        copies = []

        def send(source, target):
            copy = pltpu.make_async_copy(source, target, sems.at[len(copies)])
            copy.start()
            copies.append(copy)

        pieces = [(ref, offset) for _, ref, offset in walk(olds[:count], rows)]
        rest = [[(ref, offset) for _, ref, offset in walk(olds[count + n * parts : count + (n + 1) * parts], half)] for n in (0, 1)]
        factors = []
        for side in (0, 1):
            square = so_ref[8 * side : 8 * side + 1, :1] + st_ref[8 * side : 8 * side + 1, :1]
            factors.append(lax.rsqrt(square / entries + 0.1))

        def product(side, start, size):
            at = pl.ds(pl.multiple_of(start, size), size)
            own, other = uo_ref[at, :], ut_ref[at, :]
            u = jnp.where(first, own, other) if side == 0 else jnp.where(first, other, own)
            return dot(u, whole[side])

        for i in range(fs_size):
            start = (fs ^ i) * rows
            block = pl.ds(pl.multiple_of(start, rows), rows)
            for side in (0, 1):
                target = spread.at[2 * i + side]
                if i == 0:
                    update = product(side, start, rows) * factors[side]
                    old = (im_ref, gm_ref)[side][...]
                    step = 0.05 * update
                    mine[2 + side] = update
                    send(mine.at[2 + side], outs[2 + side])
                    mine[side] = old - step
                    send(mine.at[side], outs[side])
                    target[...] = (old.astype(BF16).astype(F32) - step).astype(BF16)
                else:
                    held_part, rest_part = pieces[i - 1], rest[side][i - 1]
                    for which, (ref, offset) in (
                        (held[side], (held_part[0], held_part[1] + side * half)),
                        (1 - held[side], rest_part),
                    ):
                        step = (0.05 * factors[side]) * product(side, start + which * half, half)
                        old = ref[offset : offset + half, :].astype(F32)
                        target[pl.ds(pl.multiple_of(which * half, half), half), :] = (old - step).astype(BF16)
                send(target, outs[4 + side].at[block, :])
        for copy in copies:
            copy.wait()

    operands = (sum_own, sum_other, normed, u_own, u_other, in_master, gate_master, *halves, *in_rest, *gate_rest)
    small, big = struct((rows, width), F32), struct((model, width), BF16)
    scratch = [
        pltpu.VMEM((4, rows, width), F32),
        pltpu.VMEM((2 * fs_size, rows, width), BF16),
        pltpu.SemaphoreType.DMA((4 + 2 * fs_size,)),
    ]
    return pl.pallas_call(
        body,
        grid_spec=one_step(operands, 6, scratch, pltpu.HBM),
        out_shape=[small, small, small, small, big, big],
        compiler_params=grant(26),
        name="finish",
    )(place, *operands)


def half_of(rep, rep_size):
    return rep & 1, (rep >> ((rep_size // 2).bit_length() - 1)) & 1


def layer(
    sizes,
    saved_input,
    cot_input,
    cot_gate,
    in_master,
    gate_master,
    in_factor,
    gate_factor,
    in_first,
    in_second,
    gate_first,
    gate_second,
):
    fs_size, rep_size, tp_size = sizes
    rows, width = in_master.shape
    part = rows // rep_size
    fs, rep, tp = (lax.axis_index(name) for name in ("fs", "rep", "tp"))
    place = jnp.stack([fs, rep, tp]).astype(jnp.int32)

    half = rows // 2

    def cut(values, index, size):
        return lax.dynamic_slice_in_dim(values, index * size, size, 0)

    def after(values, *others):
        return lax.optimization_barrier((values, *others))[0]

    sent = jnp.where(tp == 0, cut(in_factor, rep, part), cut(gate_factor, rep, part))
    direct = from_others(sent, "fs", fs_size)
    x = stage(saved_input)
    relayed = from_others(jnp.concatenate(direct, axis=0), "rep", rep_size)

    held = half_of(rep, rep_size)
    old = [cut(values, index, half) for values, index in zip((in_master, gate_master), held)]
    old = after(jnp.concatenate(old, axis=0).astype(BF16), *direct)
    if fs_size == 4:
        near = swap(old, "fs", fs_size, 1)
        far = swap(old, "fs", fs_size, 2)
        halves = [near, far]
    else:
        halves = from_others(old, "fs", fs_size)

    def rest_of(values, cue):
        ready = [piece.reshape(-1, 2, half, width) for piece in lax.optimization_barrier((*values, cue))[:-1]]
        return [
            swap(jnp.concatenate([piece[:, side].reshape(-1, width) for piece in ready]), "rep", rep_size, step)
            for side, step in ((0, 1), (1, rep_size // 2))
        ]

    y_own, u_own = project(place, x, in_factor, gate_factor, direct, relayed, rep_size)
    y_other = swap(y_own, "tp", tp_size, 1)
    u_other = swap(u_own, "tp", tp_size, 1)
    sums = token_sums(place, y_own, y_other, cot_input, cot_gate, rep_size)
    parts = [sums[0]] + [swap(sums[j], "rep", rep_size, j) for j in range(1, rep_size)]
    products = gram(place, after(u_own, sums[-1]), u_other)
    sums = add_up(place, parts, fs_size)
    if fs_size <= DIRECT:
        parts = [sums[0]] + [swap(sums[k], "fs", fs_size, k) for k in range(1, fs_size)]
    else:
        parts = [lax.psum_scatter(sums[0], "fs", scatter_dimension=0, tiled=True)]
    state = (in_first, in_second, gate_first, gate_second)
    low, normed = norm_block(place, parts, *state)
    column = jnp.concatenate([normed, *from_others(normed, "fs", fs_size), low], axis=0)
    rest = [rest_of(halves, sums[-1])]
    if fs_size == 4:
        halves.append(swap(after(far, normed), "fs", fs_size, 1))
        rest.append(rest_of(halves[2:], column))
    blocks = [column] + from_others(column, "rep", rep_size)
    whole, sum_own = squares(place, blocks, products, fs_size, width)
    sum_other = swap(sum_own, "tp", tp_size, 1)
    new = moments(place, after(blocks[0], sum_own), blocks[1:], *state)
    entries = float(rows * fs_size * width * tp_size)
    in_rest, gate_rest = zip(*rest)
    olds = (in_master, gate_master, halves, in_rest, gate_rest)
    head = finish(place, sum_own, sum_other, whole, u_own, u_other, *olds, rep_size, entries)
    return (*head[:4], *new, *head[4:])


def solution(mesh):
    sizes = tuple(mesh.shape[name] for name in ("fs", "rep", "tp"))
    owned, moment = P("fs", "tp"), P("fs", "tp")
    return jax.shard_map(
        functools.partial(layer, sizes),
        mesh=mesh,
        in_specs=(
            P(("fs", "rep"), None),
            P(("fs", "rep"), "tp"),
            P(("fs", "rep"), "tp"),
            owned,
            owned,
            P("fs", None),
            P("fs", None),
            moment,
            moment,
            moment,
            moment,
        ),
        out_specs=(owned,) * 4 + (moment,) * 4 + (P(None, "tp"),) * 2,
        check_vma=False,
    )
```

```python
import functools

import jax
import jax.numpy as jnp
from jax import lax
from jax.experimental import pallas as pl
from jax.experimental.pallas import tpu as pltpu
from jax.sharding import PartitionSpec as P


F32 = jnp.float32
BF16 = jnp.bfloat16
DIRECT = 4
CONTRACT_ROWS = (((0,), (0,)), ((), ()))


def dot(left, right):
    return jnp.dot(left, right, preferred_element_type=F32)


def swap(values, axis, size, step):
    return lax.ppermute(values, axis, [(i, i ^ step) for i in range(size)])


def from_others(values, axis, size):
    if size <= DIRECT:
        return [swap(values, axis, size, k) for k in range(1, size)]
    whole = lax.all_gather(values, axis)
    order = lax.axis_index(axis) ^ jnp.arange(1, size)
    return [jnp.take(whole, order, axis=0).reshape((-1, *values.shape[1:]))]


def one_step(operands, n_outs, scratch=(), out_space=pltpu.VMEM):
    return pltpu.PrefetchScalarGridSpec(
        num_scalar_prefetch=1,
        grid=(),
        in_specs=[pl.BlockSpec(memory_space=pltpu.VMEM)] * len(operands),
        out_specs=[pl.BlockSpec(memory_space=out_space)] * n_outs,
        scratch_shapes=scratch,
    )


def grant(mib):
    return pltpu.CompilerParams(vmem_limit_bytes=mib << 20)


def struct(shape, kind):
    return jax.ShapeDtypeStruct(shape, kind)


def walk(refs, rows):
    k = 0
    for ref in refs:
        for offset in range(0, ref.shape[0], rows):
            k += 1
            yield k, ref, offset


def stage(values):
    def body(in_ref, out_ref, sem):
        copy = pltpu.make_async_copy(in_ref, out_ref, sem)
        copy.start()
        copy.wait()

    return pl.pallas_call(
        body,
        in_specs=[pl.BlockSpec(memory_space=pltpu.HBM)],
        out_specs=pl.BlockSpec(memory_space=pltpu.VMEM),
        out_shape=struct(values.shape, values.dtype),
        scratch_shapes=[pltpu.SemaphoreType.DMA],
        compiler_params=grant(10),
        name="stage",
    )(values)


def held_rows(place, masters, rep_size):
    rows, width = masters[0].shape
    half = rows // 2

    def body(place_ref, in_ref, gate_ref, out_ref):
        is_in = place_ref[2] == 0
        for side, which in enumerate(half_of(place_ref[1], rep_size)):
            at = pl.ds(pl.multiple_of(which * half, half), half)
            wanted = jnp.where(is_in if side == 0 else jnp.logical_not(is_in), in_ref[at, :], gate_ref[at, :])
            out_ref[side * half : (side + 1) * half, :] = wanted.astype(BF16)

    return pl.pallas_call(
        body,
        grid_spec=one_step(masters, 1),
        out_shape=[struct((rows, width), BF16)],
        compiler_params=grant(6),
        name="held_rows",
    )(place, *masters)[0]


def project(place, x, in_factor, gate_factor, direct, relayed, rep_size):
    tokens, model = x.shape
    rows, rank = in_factor.shape
    part = rows // rep_size
    n_direct = len(direct)

    def body(place_ref, x_ref, in_ref, gate_ref, *refs):
        pieces, (y_ref, whole_ref) = refs[:-2], refs[-2:]
        fs, rep = place_ref[0], place_ref[1]
        own = jnp.where(place_ref[2] == 0, in_ref[...], gate_ref[...])
        whole_ref[pl.ds(pl.multiple_of(fs * rows, rows), rows), :] = own
        groups = [(0, pieces[:n_direct])]
        groups += [(j + 1, [piece]) for j, piece in enumerate(pieces[n_direct:])]
        for j, group in groups:
            for k, ref, offset in walk(group, part):
                start = pl.multiple_of((fs ^ k) * rows + (rep ^ j) * part, part)
                whole_ref[pl.ds(start, part), :] = ref[offset : offset + part, :]
        y_ref[...] = dot(x_ref[...], whole_ref[...]).astype(BF16)

    operands = (x, in_factor, gate_factor, *direct, *relayed)
    return pl.pallas_call(
        body,
        grid_spec=one_step(operands, 2),
        out_shape=[struct((tokens, rank), BF16), struct((model, rank), BF16)],
        compiler_params=grant(12),
        name="project",
    )(place, *operands)


def token_sums(place, y, cotangents, rep_size):
    rank = y.shape[1]
    width = cotangents[0].shape[1]
    per = rep_size // 2
    columns = width // per

    def body(place_ref, y_ref, ci, cg, other_ci, other_cg, *refs):
        outs, scratch = refs[:-1], refs[-1]
        core = place_ref[2]
        halves = [jnp.where(core == 0, a[...], b[...]) for a, b in ((ci, cg), (other_ci, other_cg))]
        sums = lax.dot_general(
            y_ref[...], jnp.concatenate(halves, axis=1), CONTRACT_ROWS, preferred_element_type=F32
        )
        for n, half in enumerate((core, 1 - core)):
            for q in range(per):
                at = (n * per + q) * columns
                scratch[half * per + q] = sums[:, at : at + columns]
        for j, out in enumerate(outs):
            out[...] = scratch[place_ref[1] ^ j].astype(out.dtype)

    outs = [struct((rank, columns), BF16 if j else F32) for j in range(rep_size)]
    operands = (y, *cotangents)
    return pl.pallas_call(
        body,
        grid_spec=one_step(operands, len(outs), [pltpu.VMEM((rep_size, rank, columns), F32)]),
        out_shape=outs,
        compiler_params=grant(10),
        name="token_sums",
    )(place, *operands)


def add_up(place, parts, fs_size):
    rank, columns = parts[0].shape
    rows = rank // fs_size
    split = fs_size <= DIRECT

    def body(place_ref, *refs):
        sums, outs, scratch = refs[: len(parts)], refs[len(parts) : -1], refs[-1]
        total = tree([ref[...].astype(F32) for ref in sums])
        if not split:
            outs[0][...] = total.astype(BF16)
            return
        for k in range(fs_size):
            scratch[k] = total[k * rows : (k + 1) * rows, :]
        for k, out in enumerate(outs):
            out[...] = scratch[place_ref[0] ^ k].astype(out.dtype)

    outs = [struct((rank, columns), BF16)]
    if split:
        outs = [struct((rows, columns), BF16 if k else F32) for k in range(fs_size)]
    return pl.pallas_call(
        body,
        grid_spec=one_step(parts, len(outs), [pltpu.VMEM((fs_size, rows, columns), F32)]),
        out_shape=outs,
        compiler_params=grant(4),
        name="add_up",
    )(place, *parts)


def tree(values):
    while len(values) > 1:
        values = [sum(values[i : i + 2][1:], values[i]) for i in range(0, len(values), 2)]
    return values[0]


def advance(first, second, low):
    return 0.8 * first + 0.2 * low, 0.95 * second + 0.05 * low * low


def norm_block(place, parts, local, remote):
    rows, columns = parts[0].shape
    width = local[0].shape[1]
    count = len(parts)

    def body(place_ref, *refs):
        sums, states, (low_ref, normed_ref) = refs[:count], refs[count:-2], refs[-2:]
        low = tree([ref[...].astype(F32) for ref in sums]).astype(BF16)
        low_ref[...] = low
        start = place_ref[1] * columns
        core = place_ref[2]
        here = (start >= width) == (core == 1)
        at = pl.ds(pl.multiple_of(lax.rem(start, width), columns), columns)
        old = []
        for n in (0, 1):
            mine, remote = (jnp.where(core == 0, states[m + n][:, at], states[m + n + 2][:, at]) for m in (0, 4))
            old.append(jnp.where(here, mine, remote))
        first, second = advance(*old, low.astype(F32))
        normed_ref[...] = (first / jnp.sqrt(second)).astype(BF16)

    operands = (*parts, *local, *remote)
    block = struct((rows, columns), BF16)
    return pl.pallas_call(
        body,
        grid_spec=one_step(operands, 2),
        out_shape=[block, block],
        compiler_params=grant(3),
        name="norm_block",
    )(place, *operands)


def flat_rows(values):
    count, rows, width = values.shape
    if rows % 16:
        return values.astype(F32).reshape(count * rows, width).astype(BF16)
    return values.reshape(count * rows, width)


def gram(u):
    model, rank = u.shape

    def body(u_ref, out_ref):
        whole = u_ref[...]
        products = lax.dot_general(whole, whole, CONTRACT_ROWS, preferred_element_type=F32)
        upper = products.astype(BF16)
        out_ref[0] = upper
        out_ref[1] = (products - upper.astype(F32)).astype(BF16)

    return pl.pallas_call(
        body,
        out_shape=struct((2, rank, rank), BF16),
        compiler_params=grant(8),
        cost_estimate=pl.CostEstimate(flops=2 * model * rank * rank, bytes_accessed=0, transcendentals=0),
        name="gram",
    )(u)


def squares(place, blocks, products, fs_size, width):
    total, columns = blocks[0].shape
    rows = total // (fs_size + 1)
    tail = 16

    def body(place_ref, *refs):
        pieces, (gram_ref, keep_ref, give_ref, scratch, low_scratch) = refs[:-5], refs[-5:]
        fs, rep, core = place_ref[0], place_ref[1], place_ref[2]
        for j, ref in enumerate(pieces):
            start = (rep ^ j) * columns
            half = start // width
            at = pl.ds(pl.multiple_of(lax.rem(start, width), columns), columns)
            for k in range(fs_size):
                scratch[half, fs ^ k, :, at] = ref[k * rows : (k + 1) * rows, :]
            low_scratch[half, :, at] = ref[-rows:, :]
        square = 0.0
        for half in (0, 1):
            part = flat_rows(scratch[half])
            image = dot(gram_ref[0], part) + dot(gram_ref[1], part)
            square = square + jnp.sum(part.astype(F32) * image)
        for out, half in ((keep_ref, core), (give_ref, 1 - core)):
            out[: fs_size * rows, :] = flat_rows(scratch[half])
            out[fs_size * rows : total, :] = low_scratch[half]
            rest = jnp.full((tail, 128), square, F32)
            for n in range(3):
                piece = rest.astype(BF16)
                out[total:, n * 128 : (n + 1) * 128] = piece
                rest = rest - piece.astype(F32)

    operands = (*blocks, products)
    out = struct((total + tail, width), BF16)
    return pl.pallas_call(
        body,
        grid_spec=one_step(
            operands,
            2,
            [pltpu.VMEM((2, fs_size, rows, width), BF16), pltpu.VMEM((2, rows, width), BF16)],
        ),
        out_shape=[out, out],
        compiler_params=grant(6),
        name="squares",
    )(place, *operands)


def locate(arrays, first, rows):
    return [(first + n, offset) for n, array in enumerate(arrays) for offset in range(0, array.shape[0], rows)]


class Side:
    def __init__(self, number, place_ref, normed_ref, factor_ref, master_refs, state_refs, old_refs, places, rep_size, entries):
        self.rows, self.width = master_refs[0].shape
        self.rank = factor_ref.shape[1]
        self.moment_rows = state_refs[0].shape[0]
        self.half = self.rows // 2
        self.fs = place_ref[0]
        self.held = half_of(place_ref[1], rep_size)[number]
        self.is_in = place_ref[2] == number
        self.normed_ref, self.factor_ref, self.master_refs, self.state_refs = normed_ref, factor_ref, master_refs, state_refs
        self.old_refs, self.places = old_refs, places
        last = self.rank + self.moment_rows
        square = sum(normed_ref[last : last + 1, n * 128 : n * 128 + 1].astype(F32) for n in (2, 1, 0))
        self.scale = lax.rsqrt(square / entries + 0.1)

    def start(self, k):
        return (self.fs ^ k) * self.rows

    def product(self, start, size):
        rows = self.factor_ref[pl.ds(pl.multiple_of(start, size), size), :]
        return dot(rows, self.normed_ref[: self.rank, :])

    def own_rows(self, update_ref, master_ref, copy_ref):
        update = self.product(self.start(0), self.rows) * self.scale
        old = jnp.where(self.is_in, self.master_refs[0][...], self.master_refs[1][...])
        step = 0.05 * update
        update_ref[...] = update
        master_ref[...] = old - step
        copy_ref[...] = (old.astype(BF16).astype(F32) - step).astype(BF16)

    def other_rows(self, k, copy_ref):
        half = self.half
        for other in (0, 1):
            which = 1 - self.held if other else self.held
            number, offset = self.places[k - 1][other]
            step = (0.05 * self.scale) * self.product(self.start(k) + which * half, half)
            old = self.old_refs[number][offset : offset + half, :].astype(F32)
            copy_ref[pl.ds(pl.multiple_of(which * half, half), half), :] = (old - step).astype(BF16)

    def moments(self, first_ref, second_ref):
        low = self.normed_ref[self.rank : self.rank + self.moment_rows, :].astype(F32)
        fi, si, fg, sg = self.state_refs
        old = [jnp.where(self.is_in, a[...], b[...]) for a, b in ((fi, fg), (si, sg))]
        first_ref[...], second_ref[...] = advance(*old, low)


def prepare(place, normed, factor, masters, state, olds, places, ready, rep_size, entries):
    rows, width = masters[0].shape
    moment_rows = state[0].shape[0]

    def body(place_ref, n_ref, u_ref, im_ref, gm_ref, fi, si, fg, sg, *refs):
        old_refs, (mine, small, spread) = refs[: len(olds)], refs[len(olds) :]
        side = Side(0, place_ref, n_ref, u_ref, (im_ref, gm_ref), (fi, si, fg, sg), old_refs, places, rep_size, entries)
        side.own_rows(mine.at[1], mine.at[0], spread.at[0])
        side.moments(small.at[0], small.at[1])
        for k in range(1, ready + 1):
            side.other_rows(k, spread.at[k])

    operands = (normed, factor, *masters, *state, *olds)
    return pl.pallas_call(
        body,
        grid_spec=one_step(operands, 3),
        out_shape=[
            struct((2, rows, width), F32),
            struct((2, moment_rows, width), F32),
            struct((ready + 1, rows, width), BF16),
        ],
        compiler_params=grant(10),
        name="prepare",
    )(place, *operands)


def finish(place, normed, factors, masters, state, olds, places, prepared, ready, rep_size, entries):
    rows, width = masters[0].shape
    model = factors[0].shape[0]
    moment_rows = state[0].shape[0]
    fs_size = model // rows
    counts = [len(arrays) for arrays in olds]

    def body(place_ref, no_ref, nt_ref, uo_ref, ut_ref, im_ref, gm_ref, fi, si, fg, sg, *refs):
        old_refs, refs = (refs[: counts[0]], refs[counts[0] : sum(counts)]), refs[sum(counts) :]
        (own_mine, own_small, own_spread), outs, (spread, mine, small, sems) = refs[:3], refs[3:13], refs[13:]
        sides = [
            Side(n, place_ref, *pair, (im_ref, gm_ref), (fi, si, fg, sg), old_refs[n], places[n], rep_size, entries)
            for n, pair in enumerate(((no_ref, uo_ref), (nt_ref, ut_ref)))
        ]
        sent = []

        def send(side, source, number, k=None):
            targets = [outs[number], outs[number + 1]]
            if k is not None:
                block = pl.ds(pl.multiple_of(side.start(k), rows), rows)
                targets = [target.at[block, :] for target in targets]
            sem = sems.at[len(sent)]
            for wanted, target in zip((side.is_in, jnp.logical_not(side.is_in)), targets):

                @pl.when(wanted)
                def _(target=target):
                    pltpu.make_async_copy(source, target, sem).start()

            sent.append(pltpu.make_async_copy(source, targets[0], sem))

        own, other = sides
        for n in (0, 1):
            send(own, own_mine.at[n], 2 * n)
        for k in range(ready + 1):
            send(own, own_spread.at[k], 8, k)
        for n in (0, 1):
            send(own, own_small.at[n], 4 + 2 * n)
        other.own_rows(mine.at[1], mine.at[0], spread.at[0])
        for n in (0, 1):
            send(other, mine.at[n], 2 * n)
        send(other, spread.at[0], 8, 0)
        other.moments(small.at[0], small.at[1])
        for n in (0, 1):
            send(other, small.at[n], 4 + 2 * n)
        for k in range(1, fs_size):
            other.other_rows(k, spread.at[k])
            send(other, spread.at[k], 8, k)
        for k in range(ready + 1, fs_size):
            own.other_rows(k, spread.at[fs_size + k - ready - 1])
            send(own, spread.at[fs_size + k - ready - 1], 8, k)
        for copy in sent:
            copy.wait()

    operands = (*normed, *factors, *masters, *state, *olds[0], *olds[1], *prepared)
    moment, owned, big = struct((moment_rows, width), F32), struct((rows, width), F32), struct((model, width), BF16)
    scratch = [
        pltpu.VMEM((2 * fs_size - ready - 1, rows, width), BF16),
        pltpu.VMEM((2, rows, width), F32),
        pltpu.VMEM((2, moment_rows, width), F32),
        pltpu.SemaphoreType.DMA((2 * (4 + fs_size),)),
    ]
    return pl.pallas_call(
        body,
        grid_spec=one_step(operands, 10, scratch, pltpu.HBM),
        out_shape=[owned] * 4 + [moment] * 4 + [big] * 2,
        compiler_params=grant(20),
        name="finish",
    )(place, *operands)


def half_of(rep, rep_size):
    return rep & 1, (rep >> ((rep_size // 2).bit_length() - 1)) & 1


def layer(
    sizes,
    saved_input,
    cot_input,
    cot_gate,
    in_master,
    gate_master,
    in_factor,
    gate_factor,
    in_first,
    in_second,
    gate_first,
    gate_second,
):
    fs_size, rep_size, tp_size = sizes
    rows, width = in_master.shape
    part = rows // rep_size
    fs, rep, tp = (lax.axis_index(name) for name in ("fs", "rep", "tp"))
    place = jnp.stack([fs, rep, tp]).astype(jnp.int32)

    half = rows // 2

    def cut(values, index, size):
        return lax.dynamic_slice_in_dim(values, index * size, size, 0)

    def after(values, *others):
        return lax.optimization_barrier((values, *others))[0]

    def own(of_in, of_gate):
        return jnp.where(tp == 0, of_in, of_gate)

    direct = from_others(own(cut(in_factor, rep, part), cut(gate_factor, rep, part)), "fs", fs_size)
    state = (in_first, in_second, gate_first, gate_second)
    cotangents = [cot_input, cot_gate]
    cotangents += [swap(after(values, *direct), "tp", tp_size, 1) for values in cotangents]
    x = stage(saved_input)
    relayed = from_others(jnp.concatenate(direct, axis=0), "rep", rep_size)

    old = held_rows(place, (in_master, gate_master), rep_size)
    if fs_size == 4:
        near = swap(old, "fs", fs_size, 1)
        far = swap(after(old, *direct), "fs", fs_size, 2)
        halves = [near, far]
    else:
        halves = from_others(old, "fs", fs_size)

    def rest_of(values, cue):
        ready = after(values, cue).reshape(-1, 2, half, width)
        return [
            swap(ready[:, side].reshape(-1, width), "rep", rep_size, step)
            for side, step in ((0, 1), (1, rep_size // 2))
        ]

    y, u_own = project(place, x, in_factor, gate_factor, direct, relayed, rep_size)
    sums = token_sums(place, y, cotangents, rep_size)
    parts = [sums[0]] + [swap(sums[j], "rep", rep_size, j) for j in range(1, rep_size)]
    u_other = swap(after(u_own, sums[-1]), "tp", tp_size, 1)
    remote_state = [swap(after(values, sums[-1]), "tp", tp_size, 1) for values in state]
    products = gram(after(u_own, sums[-1]))
    rest = rest_of(halves[0], sums[-1])
    sums = add_up(place, parts, fs_size)
    if fs_size <= DIRECT:
        parts = [sums[0]] + [swap(sums[k], "fs", fs_size, k) for k in range(1, fs_size)]
    else:
        parts = [lax.psum_scatter(sums[0], "fs", scatter_dimension=0, tiled=True)]
    low, normed = norm_block(place, parts, state, remote_state)
    column = jnp.concatenate([normed, *from_others(normed, "fs", fs_size), low], axis=0)
    if fs_size == 4:
        rest += rest_of(far, sums[-1])
        last = [swap(after(far, sums[-1])[:half], "fs", fs_size, 1)]
        last.append(swap(after(far, normed)[half:], "fs", fs_size, 1))
        last_rest = [swap(after(last[0], column), "rep", rep_size, 1)]
        last_rest.append(swap(after(last[1], column), "rep", rep_size, rep_size // 2))
    blocks = [column] + from_others(column, "rep", rep_size)
    kept, given = squares(place, blocks, products, fs_size, width)
    got = swap(given, "tp", tp_size, 1)

    entries = float(rows * fs_size * width * tp_size)
    masters = (in_master, gate_master)
    if fs_size == 4:
        ready = 2
        olds = [[near, far, rest[side], rest[2 + side], last[side], last_rest[side]] for side in (0, 1)]
        places = [[[(0, side * half), (2, 0)], [(1, side * half), (3, 0)], [(4, 0), (5, 0)]] for side in (0, 1)]
    else:
        ready = 0
        olds = [[*halves, *rest[side::2]] for side in (0, 1)]
        found = [(locate(halves, 0, half)[side::2], locate(rest[side::2], len(halves), half)) for side in (0, 1)]
        places = [list(zip(*pair)) for pair in found]
    early = olds[0][: 2 * ready]
    prepared = prepare(place, kept, u_own, masters, state, early, places[0], ready, rep_size, entries)
    outs = finish(
        place, (kept, got), (u_own, u_other), masters, state, olds, places, prepared, ready, rep_size, entries
    )
    order = (0, 1, 2, 3, 4, 6, 5, 7, 8, 9)
    return tuple(outs[n] for n in order)


def solution(mesh):
    sizes = tuple(mesh.shape[name] for name in ("fs", "rep", "tp"))
    owned, moment = P("fs", "tp"), P("fs", "tp")
    return jax.shard_map(
        functools.partial(layer, sizes),
        mesh=mesh,
        in_specs=(
            P(("fs", "rep"), None),
            P(("fs", "rep"), "tp"),
            P(("fs", "rep"), "tp"),
            owned,
            owned,
            P("fs", None),
            P("fs", None),
            moment,
            moment,
            moment,
            moment,
        ),
        out_specs=(owned,) * 4 + (moment,) * 4 + (P(None, "tp"),) * 2,
        check_vma=False,
    )
```

```python
import functools

import jax
import jax.numpy as jnp
from jax import lax
from jax.experimental import pallas as pl
from jax.experimental.pallas import tpu as pltpu
from jax.sharding import PartitionSpec as P


F32 = jnp.float32
BF16 = jnp.bfloat16
DIRECT = 4
CONTRACT_ROWS = (((0,), (0,)), ((), ()))


def dot(left, right):
    return jnp.dot(left, right, preferred_element_type=F32)


def swap(values, axis, size, step):
    return lax.ppermute(values, axis, [(i, i ^ step) for i in range(size)])


def from_others(values, axis, size):
    if size <= DIRECT:
        return [swap(values, axis, size, k) for k in range(1, size)]
    whole = lax.all_gather(values, axis)
    order = lax.axis_index(axis) ^ jnp.arange(1, size)
    return [jnp.take(whole, order, axis=0).reshape((-1, *values.shape[1:]))]


def one_step(operands, n_outs, scratch=(), out_space=pltpu.VMEM):
    return pltpu.PrefetchScalarGridSpec(
        num_scalar_prefetch=1,
        grid=(),
        in_specs=[pl.BlockSpec(memory_space=pltpu.VMEM)] * len(operands),
        out_specs=[pl.BlockSpec(memory_space=out_space)] * n_outs,
        scratch_shapes=scratch,
    )


def grant(mib):
    return pltpu.CompilerParams(vmem_limit_bytes=mib << 20)


def struct(shape, kind):
    return jax.ShapeDtypeStruct(shape, kind)


def walk(refs, rows):
    k = 0
    for ref in refs:
        for offset in range(0, ref.shape[0], rows):
            k += 1
            yield k, ref, offset


def stage(values):
    def body(in_ref, out_ref, sem):
        copy = pltpu.make_async_copy(in_ref, out_ref, sem)
        copy.start()
        copy.wait()

    return pl.pallas_call(
        body,
        in_specs=[pl.BlockSpec(memory_space=pltpu.HBM)],
        out_specs=pl.BlockSpec(memory_space=pltpu.VMEM),
        out_shape=struct(values.shape, values.dtype),
        scratch_shapes=[pltpu.SemaphoreType.DMA],
        compiler_params=grant(10),
        name="stage",
    )(values)


def held_rows(place, masters, rep_size):
    rows, width = masters[0].shape
    half = rows // 2

    def body(place_ref, in_ref, gate_ref, out_ref):
        is_in = place_ref[2] == 0
        for side, which in enumerate(half_of(place_ref[1], rep_size)):
            at = pl.ds(pl.multiple_of(which * half, half), half)
            wanted = jnp.where(is_in if side == 0 else jnp.logical_not(is_in), in_ref[at, :], gate_ref[at, :])
            out_ref[side * half : (side + 1) * half, :] = wanted.astype(BF16)

    return pl.pallas_call(
        body,
        grid_spec=one_step(masters, 1),
        out_shape=[struct((rows, width), BF16)],
        compiler_params=grant(6),
        name="held_rows",
    )(place, *masters)[0]


def project(place, x, in_factor, gate_factor, direct, relayed, rep_size):
    tokens, model = x.shape
    rows, rank = in_factor.shape
    part = rows // rep_size
    n_direct = len(direct)

    def body(place_ref, x_ref, in_ref, gate_ref, *refs):
        pieces, (y_ref, whole_ref) = refs[:-2], refs[-2:]
        fs, rep = place_ref[0], place_ref[1]
        own = jnp.where(place_ref[2] == 0, in_ref[...], gate_ref[...])
        whole_ref[pl.ds(pl.multiple_of(fs * rows, rows), rows), :] = own
        groups = [(0, pieces[:n_direct])]
        groups += [(j + 1, [piece]) for j, piece in enumerate(pieces[n_direct:])]
        for j, group in groups:
            for k, ref, offset in walk(group, part):
                start = pl.multiple_of((fs ^ k) * rows + (rep ^ j) * part, part)
                whole_ref[pl.ds(start, part), :] = ref[offset : offset + part, :]
        y_ref[...] = dot(x_ref[...], whole_ref[...]).astype(BF16)

    operands = (x, in_factor, gate_factor, *direct, *relayed)
    return pl.pallas_call(
        body,
        grid_spec=one_step(operands, 2),
        out_shape=[struct((tokens, rank), BF16), struct((model, rank), BF16)],
        compiler_params=grant(12),
        name="project",
    )(place, *operands)


def token_sums(place, y, cotangents, rep_size):
    rank = y.shape[1]
    width = cotangents[0].shape[1]
    per = rep_size // 2
    columns = width // per

    def body(place_ref, y_ref, ci, cg, other_ci, other_cg, *refs):
        outs, scratch = refs[:-1], refs[-1]
        core = place_ref[2]
        halves = [jnp.where(core == 0, a[...], b[...]) for a, b in ((ci, cg), (other_ci, other_cg))]
        sums = lax.dot_general(
            y_ref[...], jnp.concatenate(halves, axis=1), CONTRACT_ROWS, preferred_element_type=F32
        )
        for n, half in enumerate((core, 1 - core)):
            for q in range(per):
                at = (n * per + q) * columns
                scratch[half * per + q] = sums[:, at : at + columns]
        for j, out in enumerate(outs):
            out[...] = scratch[place_ref[1] ^ j].astype(out.dtype)

    outs = [struct((rank, columns), BF16 if j else F32) for j in range(rep_size)]
    operands = (y, *cotangents)
    return pl.pallas_call(
        body,
        grid_spec=one_step(operands, len(outs), [pltpu.VMEM((rep_size, rank, columns), F32)]),
        out_shape=outs,
        compiler_params=grant(10),
        name="token_sums",
    )(place, *operands)


def add_up(place, parts, fs_size):
    rank, columns = parts[0].shape
    rows = rank // fs_size
    split = fs_size <= DIRECT

    def body(place_ref, *refs):
        sums, outs, scratch = refs[: len(parts)], refs[len(parts) : -1], refs[-1]
        total = tree([ref[...].astype(F32) for ref in sums])
        if not split:
            outs[0][...] = total.astype(BF16)
            return
        for k in range(fs_size):
            scratch[k] = total[k * rows : (k + 1) * rows, :]
        for k, out in enumerate(outs):
            out[...] = scratch[place_ref[0] ^ k].astype(out.dtype)

    outs = [struct((rank, columns), BF16)]
    if split:
        outs = [struct((rows, columns), BF16 if k else F32) for k in range(fs_size)]
    return pl.pallas_call(
        body,
        grid_spec=one_step(parts, len(outs), [pltpu.VMEM((fs_size, rows, columns), F32)]),
        out_shape=outs,
        compiler_params=grant(4),
        name="add_up",
    )(place, *parts)


def tree(values):
    while len(values) > 1:
        values = [sum(values[i : i + 2][1:], values[i]) for i in range(0, len(values), 2)]
    return values[0]


def advance(first, second, low):
    return 0.8 * first + 0.2 * low, 0.95 * second + 0.05 * low * low


def normalize(first, second):
    return (first / jnp.sqrt(second)).astype(BF16)


def norm_block(place, parts, local, remote):
    rows, columns = parts[0].shape
    width = local[0].shape[1]
    count = len(parts)

    def body(place_ref, *refs):
        sums, states, (low_ref, normed_ref) = refs[:count], refs[count:-2], refs[-2:]
        low = tree([ref[...].astype(F32) for ref in sums]).astype(BF16)
        low_ref[...] = low
        start = place_ref[1] * columns
        core = place_ref[2]
        here = (start >= width) == (core == 1)
        at = pl.ds(pl.multiple_of(lax.rem(start, width), columns), columns)
        old = []
        for n in (0, 1):
            mine, remote = (jnp.where(core == 0, states[m + n][:, at], states[m + n + 2][:, at]) for m in (0, 4))
            old.append(jnp.where(here, mine, remote))
        first, second = advance(*old, low.astype(F32))
        normed_ref[...] = normalize(first, second)

    operands = (*parts, *local, *remote)
    block = struct((rows, columns), BF16)
    return pl.pallas_call(
        body,
        grid_spec=one_step(operands, 2),
        out_shape=[block, block],
        compiler_params=grant(3),
        name="norm_block",
    )(place, *operands)


def flat_rows(values):
    count, rows, width = values.shape
    if rows % 16:
        return values.astype(F32).reshape(count * rows, width).astype(BF16)
    return values.reshape(count * rows, width)


def gram(u):
    model, rank = u.shape

    def body(u_ref, out_ref):
        whole = u_ref[...]
        products = lax.dot_general(whole, whole, CONTRACT_ROWS, preferred_element_type=F32)
        upper = products.astype(BF16)
        out_ref[0] = upper
        out_ref[1] = (products - upper.astype(F32)).astype(BF16)

    return pl.pallas_call(
        body,
        out_shape=struct((2, rank, rank), BF16),
        compiler_params=grant(8),
        cost_estimate=pl.CostEstimate(flops=2 * model * rank * rank, bytes_accessed=0, transcendentals=0),
        name="gram",
    )(u)


def squares(place, blocks, products, local, remote, fs_size):
    rank, columns = blocks[0].shape
    rows, width = local[0].shape
    total = rank + rows
    tail = 16
    count = len(blocks)

    def body(place_ref, *refs):
        pieces, states, (gram_ref, keep_ref, give_ref, scratch, low_scratch) = refs[:count], refs[count:-5], refs[-5:]
        fs, rep, core = place_ref[0], place_ref[1], place_ref[2]
        for j, ref in enumerate(pieces):
            start = (rep ^ j) * columns
            half = start // width
            at = pl.ds(pl.multiple_of(lax.rem(start, width), columns), columns)
            low_scratch[half, :, at] = ref[:rows, :]
            for k in range(1, fs_size):
                scratch[half, fs ^ k, :, at] = ref[k * rows : (k + 1) * rows, :]
        for half, first in ((core, 0), (1 - core, 4)):
            old = [jnp.where(core == 0, states[first + n][...], states[first + n + 2][...]) for n in (0, 1)]
            new = advance(*old, low_scratch[half].astype(F32))
            scratch[half, fs] = normalize(*new)
        square = 0.0
        for half in (0, 1):
            part = flat_rows(scratch[half])
            image = dot(gram_ref[0], part) + dot(gram_ref[1], part)
            square = square + jnp.sum(part.astype(F32) * image)
        for out, half in ((keep_ref, core), (give_ref, 1 - core)):
            out[:rank, :] = flat_rows(scratch[half])
            out[rank:total, :] = low_scratch[half]
            rest = jnp.full((tail, 128), square, F32)
            for n in range(3):
                piece = rest.astype(BF16)
                out[total:, n * 128 : (n + 1) * 128] = piece
                rest = rest - piece.astype(F32)

    operands = (*blocks, *local, *remote, products)
    out = struct((total + tail, width), BF16)
    return pl.pallas_call(
        body,
        grid_spec=one_step(
            operands,
            2,
            [pltpu.VMEM((2, fs_size, rows, width), BF16), pltpu.VMEM((2, rows, width), BF16)],
        ),
        out_shape=[out, out],
        compiler_params=grant(6),
        name="squares",
    )(place, *operands)


def locate(arrays, first, rows):
    return [(first + n, offset) for n, array in enumerate(arrays) for offset in range(0, array.shape[0], rows)]


class Side:
    def __init__(self, number, place_ref, normed_ref, factor_ref, master_refs, state_refs, old_refs, places, rep_size, entries):
        self.rows, self.width = master_refs[0].shape
        self.rank = factor_ref.shape[1]
        self.moment_rows = state_refs[0].shape[0]
        self.half = self.rows // 2
        self.fs = place_ref[0]
        self.held = half_of(place_ref[1], rep_size)[number]
        self.is_in = place_ref[2] == number
        self.normed_ref, self.factor_ref, self.master_refs, self.state_refs = normed_ref, factor_ref, master_refs, state_refs
        self.old_refs, self.places = old_refs, places
        last = self.rank + self.moment_rows
        square = sum(normed_ref[last : last + 1, n * 128 : n * 128 + 1].astype(F32) for n in (2, 1, 0))
        self.scale = lax.rsqrt(square / entries + 0.1)

    def start(self, k):
        return (self.fs ^ k) * self.rows

    def product(self, start, size):
        rows = self.factor_ref[pl.ds(pl.multiple_of(start, size), size), :]
        return dot(rows, self.normed_ref[: self.rank, :])

    def own_rows(self, update_ref, master_ref, copy_ref):
        update = self.product(self.start(0), self.rows) * self.scale
        old = jnp.where(self.is_in, self.master_refs[0][...], self.master_refs[1][...])
        step = 0.05 * update
        update_ref[...] = update
        master_ref[...] = old - step
        copy_ref[...] = (old.astype(BF16).astype(F32) - step).astype(BF16)

    def other_rows(self, k, copy_ref):
        half = self.half
        for other in (0, 1):
            which = 1 - self.held if other else self.held
            number, offset = self.places[k - 1][other]
            step = (0.05 * self.scale) * self.product(self.start(k) + which * half, half)
            old = self.old_refs[number][offset : offset + half, :].astype(F32)
            copy_ref[pl.ds(pl.multiple_of(which * half, half), half), :] = (old - step).astype(BF16)

    def moments(self, first_ref, second_ref):
        low = self.normed_ref[self.rank : self.rank + self.moment_rows, :].astype(F32)
        fi, si, fg, sg = self.state_refs
        old = [jnp.where(self.is_in, a[...], b[...]) for a, b in ((fi, fg), (si, sg))]
        first_ref[...], second_ref[...] = advance(*old, low)


def prepare(place, normed, factor, masters, state, olds, places, ready, rep_size, entries):
    rows, width = masters[0].shape
    moment_rows = state[0].shape[0]

    def body(place_ref, n_ref, u_ref, im_ref, gm_ref, fi, si, fg, sg, *refs):
        old_refs, (mine, small, spread) = refs[: len(olds)], refs[len(olds) :]
        side = Side(0, place_ref, n_ref, u_ref, (im_ref, gm_ref), (fi, si, fg, sg), old_refs, places, rep_size, entries)
        side.own_rows(mine.at[1], mine.at[0], spread.at[0])
        side.moments(small.at[0], small.at[1])
        for k in range(1, ready + 1):
            side.other_rows(k, spread.at[k])

    operands = (normed, factor, *masters, *state, *olds)
    return pl.pallas_call(
        body,
        grid_spec=one_step(operands, 3),
        out_shape=[
            struct((2, rows, width), F32),
            struct((2, moment_rows, width), F32),
            struct((ready + 1, rows, width), BF16),
        ],
        compiler_params=grant(10),
        name="prepare",
    )(place, *operands)


def finish(place, normed, factors, masters, state, olds, places, prepared, ready, rep_size, entries):
    rows, width = masters[0].shape
    model = factors[0].shape[0]
    moment_rows = state[0].shape[0]
    fs_size = model // rows
    counts = [len(arrays) for arrays in olds]

    def body(place_ref, no_ref, nt_ref, uo_ref, ut_ref, im_ref, gm_ref, fi, si, fg, sg, *refs):
        old_refs, refs = (refs[: counts[0]], refs[counts[0] : sum(counts)]), refs[sum(counts) :]
        (own_mine, own_small, own_spread), outs, (spread, mine, small, sems) = refs[:3], refs[3:13], refs[13:]
        sides = [
            Side(n, place_ref, *pair, (im_ref, gm_ref), (fi, si, fg, sg), old_refs[n], places[n], rep_size, entries)
            for n, pair in enumerate(((no_ref, uo_ref), (nt_ref, ut_ref)))
        ]
        sent = []

        def send(side, source, number, k=None):
            targets = [outs[number], outs[number + 1]]
            if k is not None:
                block = pl.ds(pl.multiple_of(side.start(k), rows), rows)
                targets = [target.at[block, :] for target in targets]
            sem = sems.at[len(sent)]
            for wanted, target in zip((side.is_in, jnp.logical_not(side.is_in)), targets):

                @pl.when(wanted)
                def _(target=target):
                    pltpu.make_async_copy(source, target, sem).start()

            sent.append(pltpu.make_async_copy(source, targets[0], sem))

        own, other = sides
        for n in (0, 1):
            send(own, own_mine.at[n], 2 * n)
        for k in range(ready + 1):
            send(own, own_spread.at[k], 8, k)
        for n in (0, 1):
            send(own, own_small.at[n], 4 + 2 * n)
        other.own_rows(mine.at[1], mine.at[0], spread.at[0])
        for n in (0, 1):
            send(other, mine.at[n], 2 * n)
        send(other, spread.at[0], 8, 0)
        other.moments(small.at[0], small.at[1])
        for n in (0, 1):
            send(other, small.at[n], 4 + 2 * n)
        for k in range(1, fs_size):
            other.other_rows(k, spread.at[k])
            send(other, spread.at[k], 8, k)
        for k in range(ready + 1, fs_size):
            own.other_rows(k, spread.at[fs_size + k - ready - 1])
            send(own, spread.at[fs_size + k - ready - 1], 8, k)
        for copy in sent:
            copy.wait()

    operands = (*normed, *factors, *masters, *state, *olds[0], *olds[1], *prepared)
    moment, owned, big = struct((moment_rows, width), F32), struct((rows, width), F32), struct((model, width), BF16)
    scratch = [
        pltpu.VMEM((2 * fs_size - ready - 1, rows, width), BF16),
        pltpu.VMEM((2, rows, width), F32),
        pltpu.VMEM((2, moment_rows, width), F32),
        pltpu.SemaphoreType.DMA((2 * (4 + fs_size),)),
    ]
    return pl.pallas_call(
        body,
        grid_spec=one_step(operands, 10, scratch, pltpu.HBM),
        out_shape=[owned] * 4 + [moment] * 4 + [big] * 2,
        compiler_params=grant(20),
        name="finish",
    )(place, *operands)


def half_of(rep, rep_size):
    return rep & 1, (rep >> ((rep_size // 2).bit_length() - 1)) & 1


def layer(
    sizes,
    saved_input,
    cot_input,
    cot_gate,
    in_master,
    gate_master,
    in_factor,
    gate_factor,
    in_first,
    in_second,
    gate_first,
    gate_second,
):
    fs_size, rep_size, tp_size = sizes
    rows, width = in_master.shape
    part = rows // rep_size
    fs, rep, tp = (lax.axis_index(name) for name in ("fs", "rep", "tp"))
    place = jnp.stack([fs, rep, tp]).astype(jnp.int32)

    half = rows // 2

    def cut(values, index, size):
        return lax.dynamic_slice_in_dim(values, index * size, size, 0)

    def after(values, *others):
        return lax.optimization_barrier((values, *others))[0]

    def own(of_in, of_gate):
        return jnp.where(tp == 0, of_in, of_gate)

    direct = from_others(own(cut(in_factor, rep, part), cut(gate_factor, rep, part)), "fs", fs_size)
    state = (in_first, in_second, gate_first, gate_second)
    cotangents = [cot_input, cot_gate]
    cotangents += [swap(after(values, *direct), "tp", tp_size, 1) for values in cotangents]
    x = stage(saved_input)
    relayed = from_others(jnp.concatenate(direct, axis=0), "rep", rep_size)

    old = held_rows(place, (in_master, gate_master), rep_size)
    if fs_size == 4:
        near = swap(old, "fs", fs_size, 1)
        far = swap(after(old, *direct), "fs", fs_size, 2)
        halves = [near, far]
    else:
        halves = from_others(old, "fs", fs_size)

    def rest_of(values, cue):
        ready = after(values, cue).reshape(-1, 2, half, width)
        return [
            swap(ready[:, side].reshape(-1, width), "rep", rep_size, step)
            for side, step in ((0, 1), (1, rep_size // 2))
        ]

    y, u_own = project(place, x, in_factor, gate_factor, direct, relayed, rep_size)
    sums = token_sums(place, y, cotangents, rep_size)
    parts = [sums[0]] + [swap(sums[j], "rep", rep_size, j) for j in range(1, rep_size)]
    u_other = swap(after(u_own, sums[-1]), "tp", tp_size, 1)
    remote_state = [swap(after(values, sums[-1]), "tp", tp_size, 1) for values in state]
    products = gram(after(u_own, sums[-1]))
    rest = rest_of(halves[0], sums[-1])
    sums = add_up(place, parts, fs_size)
    if fs_size <= DIRECT:
        parts = [sums[0]] + [swap(sums[k], "fs", fs_size, k) for k in range(1, fs_size)]
    else:
        parts = [lax.psum_scatter(sums[0], "fs", scatter_dimension=0, tiled=True)]
    low, normed = norm_block(place, parts, state, remote_state)
    column = jnp.concatenate([low, *from_others(normed, "fs", fs_size)], axis=0)
    if fs_size == 4:
        rest += rest_of(far, sums[-1])
        last = [swap(after(far, sums[-1])[:half], "fs", fs_size, 1)]
        last.append(swap(after(far, normed)[half:], "fs", fs_size, 1))
        last_rest = [swap(after(last[0], column), "rep", rep_size, 1)]
        last_rest.append(swap(after(last[1], column), "rep", rep_size, rep_size // 2))
    blocks = [column] + from_others(column, "rep", rep_size)
    kept, given = squares(place, blocks, products, state, remote_state, fs_size)
    got = swap(given, "tp", tp_size, 1)

    entries = float(rows * fs_size * width * tp_size)
    masters = (in_master, gate_master)
    if fs_size == 4:
        ready = 2
        olds = [[near, far, rest[side], rest[2 + side], last[side], last_rest[side]] for side in (0, 1)]
        places = [[[(0, side * half), (2, 0)], [(1, side * half), (3, 0)], [(4, 0), (5, 0)]] for side in (0, 1)]
    else:
        ready = 0
        olds = [[*halves, *rest[side::2]] for side in (0, 1)]
        found = [(locate(halves, 0, half)[side::2], locate(rest[side::2], len(halves), half)) for side in (0, 1)]
        places = [list(zip(*pair)) for pair in found]
    early = olds[0][: 2 * ready]
    prepared = prepare(place, kept, u_own, masters, state, early, places[0], ready, rep_size, entries)
    outs = finish(
        place, (kept, got), (u_own, u_other), masters, state, olds, places, prepared, ready, rep_size, entries
    )
    order = (0, 1, 2, 3, 4, 6, 5, 7, 8, 9)
    return tuple(outs[n] for n in order)


def solution(mesh):
    sizes = tuple(mesh.shape[name] for name in ("fs", "rep", "tp"))
    owned, moment = P("fs", "tp"), P("fs", "tp")
    return jax.shard_map(
        functools.partial(layer, sizes),
        mesh=mesh,
        in_specs=(
            P(("fs", "rep"), None),
            P(("fs", "rep"), "tp"),
            P(("fs", "rep"), "tp"),
            owned,
            owned,
            P("fs", None),
            P("fs", None),
            moment,
            moment,
            moment,
            moment,
        ),
        out_specs=(owned,) * 4 + (moment,) * 4 + (P(None, "tp"),) * 2,
        check_vma=False,
    )
```

```python
import functools

import jax
import jax.numpy as jnp
from jax import lax
from jax.experimental import pallas as pl
from jax.experimental.pallas import tpu as pltpu
from jax.sharding import PartitionSpec as P


F32 = jnp.float32
BF16 = jnp.bfloat16
DIRECT = 4
CONTRACT_ROWS = (((0,), (0,)), ((), ()))


def dot(left, right):
    return jnp.dot(left, right, preferred_element_type=F32)


def swap(values, axis, size, step):
    return lax.ppermute(values, axis, [(i, i ^ step) for i in range(size)])


def to_others(blocks, axis, size):
    arrived = []
    for k in range(1, size):
        arrived.append(swap(blocks[k], axis, size, k))
    return arrived


def from_others(values, axis, size):
    if size <= DIRECT:
        return to_others([values] * size, axis, size)
    whole = lax.all_gather(values, axis)
    order = lax.axis_index(axis) ^ jnp.arange(1, size)
    return [jnp.take(whole, order, axis=0).reshape((-1, *values.shape[1:]))]


def one_step(operands, n_outs, scratch=(), out_space=pltpu.VMEM):
    return pltpu.PrefetchScalarGridSpec(
        num_scalar_prefetch=1,
        grid=(),
        in_specs=[pl.BlockSpec(memory_space=pltpu.VMEM)] * len(operands),
        out_specs=[pl.BlockSpec(memory_space=out_space)] * n_outs,
        scratch_shapes=scratch,
    )


def grant(mib):
    return pltpu.CompilerParams(vmem_limit_bytes=mib << 20)


def struct(shape, kind):
    return jax.ShapeDtypeStruct(shape, kind)


def walk(refs, rows):
    k = 0
    for ref in refs:
        for offset in range(0, ref.shape[0], rows):
            k += 1
            yield k, ref, offset


def stage(values):
    def body(in_ref, out_ref, sem):
        copy = pltpu.make_async_copy(in_ref, out_ref, sem)
        copy.start()
        copy.wait()

    return pl.pallas_call(
        body,
        in_specs=[pl.BlockSpec(memory_space=pltpu.HBM)],
        out_specs=pl.BlockSpec(memory_space=pltpu.VMEM),
        out_shape=struct(values.shape, values.dtype),
        scratch_shapes=[pltpu.SemaphoreType.DMA],
        compiler_params=grant(10),
        name="stage",
    )(values)


def held_rows(place, masters, rep_size):
    rows, width = masters[0].shape
    half = rows // 2

    def body(place_ref, in_ref, gate_ref, out_ref):
        is_in = place_ref[2] == 0
        for side, which in enumerate(half_of(place_ref[1], rep_size)):
            at = pl.ds(pl.multiple_of(which * half, half), half)
            wanted = jnp.where(is_in if side == 0 else jnp.logical_not(is_in), in_ref[at, :], gate_ref[at, :])
            out_ref[side * half : (side + 1) * half, :] = wanted.astype(BF16)

    return pl.pallas_call(
        body,
        grid_spec=one_step(masters, 1),
        out_shape=[struct((rows, width), BF16)],
        compiler_params=grant(6),
        name="held_rows",
    )(place, *masters)[0]


def project(place, x, in_factor, gate_factor, direct, relayed, rep_size):
    tokens, model = x.shape
    rows, rank = in_factor.shape
    part = rows // rep_size
    n_direct = len(direct)

    def body(place_ref, x_ref, in_ref, gate_ref, *refs):
        pieces, (y_ref, whole_ref) = refs[:-2], refs[-2:]
        fs, rep = place_ref[0], place_ref[1]
        own = jnp.where(place_ref[2] == 0, in_ref[...], gate_ref[...])
        whole_ref[pl.ds(pl.multiple_of(fs * rows, rows), rows), :] = own
        groups = [(0, pieces[:n_direct])]
        groups += [(j + 1, [piece]) for j, piece in enumerate(pieces[n_direct:])]
        for j, group in groups:
            for k, ref, offset in walk(group, part):
                start = pl.multiple_of((fs ^ k) * rows + (rep ^ j) * part, part)
                whole_ref[pl.ds(start, part), :] = ref[offset : offset + part, :]
        y_ref[...] = dot(x_ref[...], whole_ref[...]).astype(BF16)

    operands = (x, in_factor, gate_factor, *direct, *relayed)
    return pl.pallas_call(
        body,
        grid_spec=one_step(operands, 2),
        out_shape=[struct((tokens, rank), BF16), struct((model, rank), BF16)],
        compiler_params=grant(12),
        name="project",
    )(place, *operands)


def token_sums(place, y, cotangents, rep_size):
    rank = y.shape[1]
    width = cotangents[0].shape[1]
    per = rep_size // 2
    columns = width // per

    def body(place_ref, y_ref, ci, cg, other_ci, other_cg, *refs):
        outs, scratch = refs[:-1], refs[-1]
        core = place_ref[2]
        halves = [jnp.where(core == 0, a[...], b[...]) for a, b in ((ci, cg), (other_ci, other_cg))]
        sums = lax.dot_general(
            y_ref[...], jnp.concatenate(halves, axis=1), CONTRACT_ROWS, preferred_element_type=F32
        )
        for n, half in enumerate((core, 1 - core)):
            for q in range(per):
                at = (n * per + q) * columns
                scratch[half * per + q] = sums[:, at : at + columns]
        for j, out in enumerate(outs):
            out[...] = scratch[place_ref[1] ^ j].astype(out.dtype)

    outs = [struct((rank, columns), BF16 if j else F32) for j in range(rep_size)]
    operands = (y, *cotangents)
    return pl.pallas_call(
        body,
        grid_spec=one_step(operands, len(outs), [pltpu.VMEM((rep_size, rank, columns), F32)]),
        out_shape=outs,
        compiler_params=grant(10),
        name="token_sums",
    )(place, *operands)


def add_up(place, parts, fs_size):
    rank, columns = parts[0].shape
    rows = rank // fs_size
    split = fs_size <= DIRECT

    def body(place_ref, *refs):
        sums, outs, scratch = refs[: len(parts)], refs[len(parts) : -1], refs[-1]
        total = tree([ref[...].astype(F32) for ref in sums])
        if not split:
            outs[0][...] = total.astype(BF16)
            return
        for k in range(fs_size):
            scratch[k] = total[k * rows : (k + 1) * rows, :]
        for k, out in enumerate(outs):
            out[...] = scratch[place_ref[0] ^ k].astype(out.dtype)

    outs = [struct((rank, columns), BF16)]
    if split:
        outs = [struct((rows, columns), BF16 if k else F32) for k in range(fs_size)]
    return pl.pallas_call(
        body,
        grid_spec=one_step(parts, len(outs), [pltpu.VMEM((fs_size, rows, columns), F32)]),
        out_shape=outs,
        compiler_params=grant(4),
        name="add_up",
    )(place, *parts)


def tree(values):
    while len(values) > 1:
        values = [sum(values[i : i + 2][1:], values[i]) for i in range(0, len(values), 2)]
    return values[0]


def advance(first, second, low):
    return 0.8 * first + 0.2 * low, 0.95 * second + 0.05 * low * low


def normalize(first, second):
    return (first * lax.rsqrt(second)).astype(BF16)


def norm_block(place, parts, local, remote):
    rows, columns = parts[0].shape
    width = local[0].shape[1]
    count = len(parts)

    def body(place_ref, *refs):
        sums, states, (low_ref, normed_ref) = refs[:count], refs[count:-2], refs[-2:]
        low = tree([ref[...].astype(F32) for ref in sums]).astype(BF16)
        low_ref[...] = low
        start = place_ref[1] * columns
        core = place_ref[2]
        here = (start >= width) == (core == 1)
        at = pl.ds(pl.multiple_of(lax.rem(start, width), columns), columns)
        old = []
        for n in (0, 1):
            mine, remote = (jnp.where(core == 0, states[m + n][:, at], states[m + n + 2][:, at]) for m in (0, 4))
            old.append(jnp.where(here, mine, remote))
        first, second = advance(*old, low.astype(F32))
        normed_ref[...] = normalize(first, second)

    operands = (*parts, *local, *remote)
    block = struct((rows, columns), BF16)
    return pl.pallas_call(
        body,
        grid_spec=one_step(operands, 2),
        out_shape=[block, block],
        compiler_params=grant(3),
        name="norm_block",
    )(place, *operands)


def flat_rows(values):
    count, rows, width = values.shape
    if rows % 16:
        return values.astype(F32).reshape(count * rows, width).astype(BF16)
    return values.reshape(count * rows, width)


def gram(u):
    model, rank = u.shape

    def body(u_ref, out_ref):
        whole = u_ref[...]
        products = lax.dot_general(whole, whole, CONTRACT_ROWS, preferred_element_type=F32)
        upper = products.astype(BF16)
        out_ref[0] = upper
        out_ref[1] = (products - upper.astype(F32)).astype(BF16)

    return pl.pallas_call(
        body,
        out_shape=struct((2, rank, rank), BF16),
        compiler_params=grant(8),
        cost_estimate=pl.CostEstimate(flops=2 * model * rank * rank, bytes_accessed=0, transcendentals=0),
        name="gram",
    )(u)


def squares(place, blocks, products, local, remote, fs_size):
    rank, columns = blocks[0].shape
    rows, width = local[0].shape
    total = rank + rows
    tail = 16
    count = len(blocks)

    def body(place_ref, *refs):
        pieces, states, (gram_ref, keep_ref, give_ref, scratch, low_scratch) = refs[:count], refs[count:-5], refs[-5:]
        fs, rep, core = place_ref[0], place_ref[1], place_ref[2]
        for j, ref in enumerate(pieces):
            start = (rep ^ j) * columns
            half = start // width
            at = pl.ds(pl.multiple_of(lax.rem(start, width), columns), columns)
            low_scratch[half, :, at] = ref[:rows, :]
            for k in range(1, fs_size):
                scratch[half, fs ^ k, :, at] = ref[k * rows : (k + 1) * rows, :]
        for half, first in ((core, 0), (1 - core, 4)):
            old = [jnp.where(core == 0, states[first + n][...], states[first + n + 2][...]) for n in (0, 1)]
            new = advance(*old, low_scratch[half].astype(F32))
            scratch[half, fs] = normalize(*new)
        square = 0.0
        for half in (0, 1):
            part = flat_rows(scratch[half])
            image = dot(gram_ref[0], part) + dot(gram_ref[1], part)
            square = square + jnp.sum(part.astype(F32) * image)
        for out, half in ((keep_ref, core), (give_ref, 1 - core)):
            out[:rank, :] = flat_rows(scratch[half])
            out[rank:total, :] = low_scratch[half]
            rest = jnp.full((tail, 128), square, F32)
            for n in range(3):
                piece = rest.astype(BF16)
                out[total:, n * 128 : (n + 1) * 128] = piece
                rest = rest - piece.astype(F32)

    operands = (*blocks, *local, *remote, products)
    out = struct((total + tail, width), BF16)
    return pl.pallas_call(
        body,
        grid_spec=one_step(
            operands,
            2,
            [pltpu.VMEM((2, fs_size, rows, width), BF16), pltpu.VMEM((2, rows, width), BF16)],
        ),
        out_shape=[out, out],
        compiler_params=grant(6),
        name="squares",
    )(place, *operands)


def locate(arrays, first, rows):
    return [(first + n, offset) for n, array in enumerate(arrays) for offset in range(0, array.shape[0], rows)]


class Side:
    def __init__(self, number, place_ref, normed_ref, factor_ref, master_refs, state_refs, old_refs, places, rep_size, entries):
        self.rows, self.width = master_refs[0].shape
        self.rank = factor_ref.shape[1]
        self.moment_rows = state_refs[0].shape[0]
        self.half = self.rows // 2
        self.fs = place_ref[0]
        self.held = half_of(place_ref[1], rep_size)[number]
        self.is_in = place_ref[2] == number
        self.normed_ref, self.factor_ref, self.master_refs, self.state_refs = normed_ref, factor_ref, master_refs, state_refs
        self.old_refs, self.places = old_refs, places
        last = self.rank + self.moment_rows
        square = sum(normed_ref[last : last + 1, n * 128 : n * 128 + 1].astype(F32) for n in (2, 1, 0))
        self.scale = lax.rsqrt(jnp.maximum(square, 0.0) / entries + 0.1)

    def start(self, k):
        return (self.fs ^ k) * self.rows

    def product(self, start, size):
        rows = self.factor_ref[pl.ds(pl.multiple_of(start, size), size), :]
        return dot(rows, self.normed_ref[: self.rank, :])

    def own_rows(self, update_ref, master_ref, copy_ref):
        update = self.product(self.start(0), self.rows) * self.scale
        old = jnp.where(self.is_in, self.master_refs[0][...], self.master_refs[1][...])
        step = 0.05 * update
        update_ref[...] = update
        master_ref[...] = old - step
        copy_ref[...] = (old.astype(BF16).astype(F32) - step).astype(BF16)

    def other_rows(self, k, copy_ref):
        half = self.half
        for other in (0, 1):
            which = 1 - self.held if other else self.held
            number, offset = self.places[k - 1][other]
            step = (0.05 * self.scale) * self.product(self.start(k) + which * half, half)
            old = self.old_refs[number][offset : offset + half, :].astype(F32)
            copy_ref[pl.ds(pl.multiple_of(which * half, half), half), :] = (old - step).astype(BF16)

    def moments(self, first_ref, second_ref):
        low = self.normed_ref[self.rank : self.rank + self.moment_rows, :].astype(F32)
        fi, si, fg, sg = self.state_refs
        old = [jnp.where(self.is_in, a[...], b[...]) for a, b in ((fi, fg), (si, sg))]
        first_ref[...], second_ref[...] = advance(*old, low)


def prepare(place, normed, factor, masters, state, olds, places, ready, rep_size, entries):
    rows, width = masters[0].shape
    moment_rows = state[0].shape[0]

    def body(place_ref, n_ref, u_ref, im_ref, gm_ref, fi, si, fg, sg, *refs):
        old_refs, (mine, small, spread) = refs[: len(olds)], refs[len(olds) :]
        side = Side(0, place_ref, n_ref, u_ref, (im_ref, gm_ref), (fi, si, fg, sg), old_refs, places, rep_size, entries)
        side.own_rows(mine.at[1], mine.at[0], spread.at[0])
        side.moments(small.at[0], small.at[1])
        for k in range(1, ready + 1):
            side.other_rows(k, spread.at[k])

    operands = (normed, factor, *masters, *state, *olds)
    return pl.pallas_call(
        body,
        grid_spec=one_step(operands, 3),
        out_shape=[
            struct((2, rows, width), F32),
            struct((2, moment_rows, width), F32),
            struct((ready + 1, rows, width), BF16),
        ],
        compiler_params=grant(10),
        name="prepare",
    )(place, *operands)


def finish(place, normed, factors, masters, state, olds, places, prepared, ready, rep_size, entries):
    rows, width = masters[0].shape
    model = factors[0].shape[0]
    moment_rows = state[0].shape[0]
    fs_size = model // rows
    counts = [len(arrays) for arrays in olds]

    def body(place_ref, no_ref, nt_ref, uo_ref, ut_ref, im_ref, gm_ref, fi, si, fg, sg, *refs):
        old_refs, refs = (refs[: counts[0]], refs[counts[0] : sum(counts)]), refs[sum(counts) :]
        (own_mine, own_small, own_spread), outs, (spread, mine, small, sems) = refs[:3], refs[3:13], refs[13:]
        sides = [
            Side(n, place_ref, *pair, (im_ref, gm_ref), (fi, si, fg, sg), old_refs[n], places[n], rep_size, entries)
            for n, pair in enumerate(((no_ref, uo_ref), (nt_ref, ut_ref)))
        ]
        sent = []

        def send(side, *jobs):
            for chosen in (0, 1):
                copies = []
                for n, (source, number, k) in enumerate(jobs):
                    target = outs[number + chosen]
                    if k is not None:
                        target = target.at[pl.ds(pl.multiple_of(side.start(k), rows), rows), :]
                    copies.append(pltpu.make_async_copy(source, target, sems.at[len(sent) + n]))

                @pl.when(side.is_in == (chosen == 0))
                def _(copies=copies):
                    for n, copy in enumerate(copies):
                        copy.start(priority=(len(sent) + n) % 2)

            sent.extend(copies)

        own, other = sides
        send(
            own,
            *((own_mine.at[n], 2 * n, None) for n in (0, 1)),
            *((own_spread.at[k], 8, k) for k in range(ready + 1)),
            *((own_small.at[n], 4 + 2 * n, None) for n in (0, 1)),
        )
        other.own_rows(mine.at[1], mine.at[0], spread.at[0])
        send(other, (mine.at[0], 0, None), (mine.at[1], 2, None), (spread.at[0], 8, 0))
        for k in range(1, fs_size):
            other.other_rows(k, spread.at[k])
            send(other, (spread.at[k], 8, k))
        for k in range(ready + 1, fs_size):
            at = fs_size + k - ready - 1
            own.other_rows(k, spread.at[at])
            send(own, (spread.at[at], 8, k))
        other.moments(small.at[0], small.at[1])
        send(other, *((small.at[n], 4 + 2 * n, None) for n in (0, 1)))
        for copy in sent:
            copy.wait()

    operands = (*normed, *factors, *masters, *state, *olds[0], *olds[1], *prepared)
    moment, owned, big = struct((moment_rows, width), F32), struct((rows, width), F32), struct((model, width), BF16)
    scratch = [
        pltpu.VMEM((2 * fs_size - ready - 1, rows, width), BF16),
        pltpu.VMEM((2, rows, width), F32),
        pltpu.VMEM((2, moment_rows, width), F32),
        pltpu.SemaphoreType.DMA((2 * (4 + fs_size),)),
    ]
    return pl.pallas_call(
        body,
        grid_spec=one_step(operands, 10, scratch, pltpu.HBM),
        out_shape=[owned] * 4 + [moment] * 4 + [big] * 2,
        compiler_params=grant(20),
        name="finish",
    )(place, *operands)


def half_of(rep, rep_size):
    return rep & 1, (rep >> ((rep_size // 2).bit_length() - 1)) & 1


def layer(
    sizes,
    saved_input,
    cot_input,
    cot_gate,
    in_master,
    gate_master,
    in_factor,
    gate_factor,
    in_first,
    in_second,
    gate_first,
    gate_second,
):
    fs_size, rep_size, tp_size = sizes
    rows, width = in_master.shape
    part = rows // rep_size
    fs, rep, tp = (lax.axis_index(name) for name in ("fs", "rep", "tp"))
    place = jnp.stack([fs, rep, tp]).astype(jnp.int32)

    half = rows // 2

    def cut(values, index, size):
        return lax.dynamic_slice_in_dim(values, index * size, size, 0)

    def after(values, *others):
        return lax.optimization_barrier((values, *others))[0]

    def own(of_in, of_gate):
        return jnp.where(tp == 0, of_in, of_gate)

    direct = from_others(own(cut(in_factor, rep, part), cut(gate_factor, rep, part)), "fs", fs_size)
    state = (in_first, in_second, gate_first, gate_second)
    cotangents = [cot_input, cot_gate]
    cotangents += [swap(after(values, *direct), "tp", tp_size, 1) for values in cotangents]
    x = stage(saved_input)
    relayed = from_others(jnp.concatenate(direct, axis=0), "rep", rep_size)

    old = held_rows(place, (in_master, gate_master), rep_size)
    if fs_size == 4:
        near = swap(old, "fs", fs_size, 1)
        far = swap(after(old, *direct), "fs", fs_size, 2)
        halves = [near, far]
    else:
        halves = from_others(old, "fs", fs_size)

    def rest_of(values, cue):
        ready = after(values, cue).reshape(-1, 2, half, width)
        return [
            swap(ready[:, side].reshape(-1, width), "rep", rep_size, step)
            for side, step in ((0, 1), (1, rep_size // 2))
        ]

    y, u_own = project(place, x, in_factor, gate_factor, direct, relayed, rep_size)
    sums = token_sums(place, y, cotangents, rep_size)
    parts = [sums[0]] + to_others(sums, "rep", rep_size)
    u_other = swap(after(u_own, sums[-1]), "tp", tp_size, 1)
    remote_state = [swap(after(values, sums[-1]), "tp", tp_size, 1) for values in state]
    products = gram(after(u_own, sums[-1]))
    rest = rest_of(halves[0], sums[-1])
    sums = add_up(place, parts, fs_size)
    if fs_size <= DIRECT:
        parts = [sums[0]] + to_others(sums, "fs", fs_size)
    else:
        parts = [lax.psum_scatter(sums[0], "fs", scatter_dimension=0, tiled=True)]
    low, normed = norm_block(place, parts, state, remote_state)
    column = jnp.concatenate([low, *from_others(normed, "fs", fs_size)], axis=0)
    if fs_size == 4:
        rest += rest_of(far, sums[-1])
        last = [swap(after(far, sums[-1])[:half], "fs", fs_size, 1)]
        last.append(swap(after(far, normed)[half:], "fs", fs_size, 1))
        last_rest = [swap(after(last[0], column), "rep", rep_size, 1)]
        last_rest.append(swap(after(last[1], column), "rep", rep_size, rep_size // 2))
    blocks = [column] + from_others(column, "rep", rep_size)
    kept, given = squares(place, blocks, products, state, remote_state, fs_size)
    got = swap(given, "tp", tp_size, 1)

    entries = float(rows * fs_size * width * tp_size)
    masters = (in_master, gate_master)
    if fs_size == 4:
        ready = 2
        olds = [[near, far, rest[side], rest[2 + side], last[side], last_rest[side]] for side in (0, 1)]
        places = [[[(0, side * half), (2, 0)], [(1, side * half), (3, 0)], [(4, 0), (5, 0)]] for side in (0, 1)]
    else:
        ready = 0
        olds = [[*halves, *rest[side::2]] for side in (0, 1)]
        found = [(locate(halves, 0, half)[side::2], locate(rest[side::2], len(halves), half)) for side in (0, 1)]
        places = [list(zip(*pair)) for pair in found]
    early = olds[0][: 2 * ready]
    prepared = prepare(place, kept, u_own, masters, state, early, places[0], ready, rep_size, entries)
    outs = finish(
        place, (kept, got), (u_own, u_other), masters, state, olds, places, prepared, ready, rep_size, entries
    )
    order = (0, 1, 2, 3, 4, 6, 5, 7, 8, 9)
    return tuple(outs[n] for n in order)


def solution(mesh):
    sizes = tuple(mesh.shape[name] for name in ("fs", "rep", "tp"))
    owned, moment = P("fs", "tp"), P("fs", "tp")
    return jax.shard_map(
        functools.partial(layer, sizes),
        mesh=mesh,
        in_specs=(
            P(("fs", "rep"), None),
            P(("fs", "rep"), "tp"),
            P(("fs", "rep"), "tp"),
            owned,
            owned,
            P("fs", None),
            P("fs", None),
            moment,
            moment,
            moment,
            moment,
        ),
        out_specs=(owned,) * 4 + (moment,) * 4 + (P(None, "tp"),) * 2,
        check_vma=False,
    )
```
